512 devices in a mesh: sp: 128 (over z, x, core), tp: 4 (over y).
Axes of the slice: x: 4, y: 4, z: 16, core: 2. Of those that a mesh axis runs over, the one named last changes fastest.
Arguments:
- tokens: bfloat16 [65536, 2048], P(('sp', 'tp')), may hold values from -6 to 6
- input_norm_scale: bfloat16 [2048], replicated, may hold values from 0.099609375 to 1.8984375
- outer_gate_weight: bfloat16 [2048, 1024], P('sp', 'tp'), may hold values from -0.125 to 0.125
- inner_gate_weight: bfloat16 [2048, 1024], P('sp', 'tp'), may hold values from -0.125 to 0.125
- value_weight_matrix: bfloat16 [2048, 1024], P('sp', 'tp'), may hold values from -0.125 to 0.125
- output_gate_weight: bfloat16 [2048, 1024], P('sp', 'tp'), may hold values from -0.125 to 0.125
- state_input_weight: bfloat16 [2048, 1024], P('sp', 'tp'), may hold values from -0.125 to 0.125
- write_key_weight: bfloat16 [2048, 512], P('sp', 'tp'), may hold values from -0.125 to 0.125
- read_key_weight: bfloat16 [2048, 512], P('sp', 'tp'), may hold values from -0.125 to 0.125
- step_size_weight: bfloat16 [2048, 16], P(None, 'tp'), may hold values from -0.125 to 0.125
- gated_conv_weight: bfloat16 [3, 1024], P(None, 'tp'), may hold values from -3.5 to 3.5
- input_conv_weight: bfloat16 [4, 1024], P(None, 'tp'), may hold values from -3 to 3
- write_conv_weight: bfloat16 [4, 512], P(None, 'tp'), may hold values from -3 to 3
- read_conv_weight: bfloat16 [4, 512], P(None, 'tp'), may hold values from -3 to 3
- step_size_bias: float32 [16], P('tp'), may hold values from -1 to 0.5
- log_decay_rate: float32 [16], P('tp'), may hold values from -16 to -2.5, as said below
- decay_spikes: float32 [16, 65536], P('tp', 'sp'), may hold values from -1 to 0, as said below
- direct_path_weight: float32 [16], P('tp'), may hold values from 0.5 to 2
- head_norm_scale: bfloat16 [1024], P('tp'), may hold values from 0.099609375 to 1.8984375
- conv_output_weight: bfloat16 [1024, 2048], P('tp', 'sp'), may hold values from -0.125 to 0.125
- state_output_weight: bfloat16 [1024, 2048], P('tp', 'sp'), may hold values from -0.125 to 0.125
Outputs:
- mixed: bfloat16 [65536, 2048], P(('sp', 'tp'))
The draws below stay inside these ranges and needn't reach their ends.
Inputs may be any that keep to these rules, and one draw needn't show every extreme that they name: `log_decay_rate`: one value a head. `decay_spikes`: never positive.
All inputs are finite; a program needn't handle non-finite values.
Results may differ from the reference program's by a relative error of at most 0.017.
Values may be sent and summed in bfloat16 or wider, within the bound.
No kernel may reach another device: no remote copies, remote signals or barrier semaphores. Data moves between devices by JAX's collectives and lax.ppermute only.
A program may use at most 128 MiB of HBM per device.

```python
import math
import jax
import jax.numpy as jnp
from jax import lax

D = 2048
CONV = 1024
MIXER_HEADS = 16
HEAD_DIM = 64
GROUPS = 4
STATE = 128
SHORT_K = 3
SSD_K = 4
BLOCK = 64
TOK_DEV = 512
INNER = 1024
SEQUENCE_TOKENS = 65536
N_TP = 4


def draw_tokens(key, part):
    positions = jnp.arange(SEQUENCE_TOKENS, dtype=jnp.int32)
    segment_ids = positions * 8 // SEQUENCE_TOKENS
    jitter_values = jax.random.truncated_normal(jax.random.fold_in(key, 31), -4.5, 4.5, (SEQUENCE_TOKENS, D), jnp.float32)
    directions = jax.random.uniform(jax.random.fold_in(key, 32), (8, D), jnp.float32, -1.2, 1.2)
    offsets = jnp.take(directions, segment_ids, axis=0)
    return (jitter_values + offsets).astype(jnp.bfloat16)


def draw_log_decay_rate(key, part):
    ranking = jax.random.permutation(jax.random.fold_in(key, 11), MIXER_HEADS)
    quick_heads = ranking < MIXER_HEADS // 2
    fast_rates = jnp.exp(jax.random.uniform(jax.random.fold_in(key, 12), (MIXER_HEADS,), jnp.float32, math.log(0.02), math.log(0.08)))
    slow_rates = jnp.exp(jax.random.uniform(jax.random.fold_in(key, 13), (MIXER_HEADS,), jnp.float32, math.log(0.1), math.log(0.3))) / SEQUENCE_TOKENS
    return jnp.log(jnp.where(quick_heads, fast_rates, slow_rates)).astype(jnp.float32)


def draw_decay_spikes(key, part):
    blocks = SEQUENCE_TOKENS // TOK_DEV
    levels = jnp.exp(jax.random.uniform(jax.random.fold_in(key, 21), (MIXER_HEADS, blocks), jnp.float32, math.log(0.25), math.log(2.0)))
    stable_decay = -0.3 / SEQUENCE_TOKENS * jnp.repeat(levels, TOK_DEV, axis=1)
    spike_positions = jax.random.randint(jax.random.fold_in(key, 22), (3,), 0, SEQUENCE_TOKENS)
    spike_present = jnp.any(jnp.arange(SEQUENCE_TOKENS)[None, :] == spike_positions[:, None], axis=0)
    spike_decrement = jax.random.uniform(jax.random.fold_in(key, 23), (MIXER_HEADS, SEQUENCE_TOKENS), jnp.float32, 0.22, 0.69)
    return (stable_decay - jnp.where(spike_present[None, :], spike_decrement, 0.0)).astype(jnp.float32)


def steps_of(own_key, dims, pieces, least, largest):
    level, own = 1.0, jax.random.fold_in(own_key, 6)
    for dim, parts in pieces:
        draws = jnp.exp(jax.random.uniform(jax.random.fold_in(own, dim), (parts,), jnp.float32, least / len(pieces), largest / len(pieces)))
        level = level * jnp.repeat(draws, dims[dim] // parts).reshape([-1 if axis == dim else 1 for axis in range(len(dims))])
    return level


def gaussian(rng, shape, deviation, limit, pieces=(), kind=jnp.bfloat16):
    drawn = jax.random.normal(rng, shape, jnp.float32) * deviation
    if len(pieces) > 0:
        drawn = steps_of(rng, shape, pieces, -0.22, 0.18) * drawn
    return jnp.clip(drawn, min=-limit, max=limit).astype(kind)


def setup_inputs(seed: int = 0) -> dict:
    streams_of = jax.random.split(jax.random.key(seed), 22)
    return {
        "tokens": draw_tokens(jax.random.fold_in(streams_of[21], 71), 0),
        "input_norm_scale": jnp.clip(1.0 + 0.18 * jax.random.normal(streams_of[1], (D,), jnp.float32), 0.099609375, 1.8984375).astype(jnp.bfloat16),
        "outer_gate_weight": gaussian(streams_of[2], (D, CONV), D ** -0.5, 0.125, ((0, 128), (1, 4))),
        "inner_gate_weight": gaussian(streams_of[3], (D, CONV), D ** -0.5, 0.125, ((0, 128), (1, 4))),
        "value_weight_matrix": gaussian(streams_of[4], (D, CONV), D ** -0.5, 0.125, ((0, 128), (1, 4))),
        "output_gate_weight": gaussian(streams_of[5], (D, INNER), D ** -0.5, 0.125, ((0, 128), (1, 4))),
        "state_input_weight": gaussian(streams_of[6], (D, INNER), D ** -0.5, 0.125, ((0, 128), (1, 4))),
        "write_key_weight": gaussian(streams_of[7], (D, GROUPS * STATE), D ** -0.5, 0.125, ((0, 128), (1, 4))),
        "read_key_weight": gaussian(streams_of[8], (D, GROUPS * STATE), D ** -0.5, 0.125, ((0, 128), (1, 4))),
        "step_size_weight": gaussian(streams_of[9], (D, MIXER_HEADS), D ** -0.5, 0.125, ((1, 4),)),
        "gated_conv_weight": gaussian(streams_of[10], (SHORT_K, CONV), SHORT_K ** -0.5, 3.5, ((1, 4),)),
        "input_conv_weight": gaussian(streams_of[11], (SSD_K, INNER), SSD_K ** -0.5, 3.0, ((1, 4),)),
        "write_conv_weight": gaussian(streams_of[12], (SSD_K, GROUPS * STATE), SSD_K ** -0.5, 3.0, ((1, 4),)),
        "read_conv_weight": gaussian(streams_of[13], (SSD_K, GROUPS * STATE), SSD_K ** -0.5, 3.0, ((1, 4),)),
        "step_size_bias": jnp.clip(-1.0 + 1.5 * jax.random.uniform(streams_of[14], (MIXER_HEADS,), jnp.float32) ** steps_of(streams_of[14], (MIXER_HEADS,), ((0, 4),), -0.2, 0.2), -1.0, 0.5),
        "log_decay_rate": draw_log_decay_rate(jax.random.fold_in(streams_of[21], 71), 0),
        "decay_spikes": draw_decay_spikes(jax.random.fold_in(streams_of[21], 71), 0),
        "direct_path_weight": jnp.clip(0.5 + 1.5 * jax.random.uniform(streams_of[17], (MIXER_HEADS,), jnp.float32) ** steps_of(streams_of[17], (MIXER_HEADS,), ((0, 4),), -0.2, 0.2), 0.5, 2.0),
        "head_norm_scale": jnp.clip(1.0 + 0.18 * jax.random.normal(streams_of[18], (INNER,), jnp.float32), 0.099609375, 1.8984375).astype(jnp.bfloat16),
        "conv_output_weight": gaussian(streams_of[19], (CONV, D), (CONV + INNER) ** -0.5, 0.125, ((0, 4), (1, 128))),
        "state_output_weight": gaussian(streams_of[20], (INNER, D), (CONV + INNER) ** -0.5, 0.125, ((0, 4), (1, 128))),
    }


epsilon = 1e-05
highest = lax.Precision.HIGHEST

def causal_taps(values, tap_weights):
    tap_count = tap_weights.shape[0]
    length = values.shape[0]
    padded = jnp.concatenate([jnp.zeros((tap_count - 1, values.shape[1]), jnp.float32), values], axis=0)
    running = tap_weights[0] * padded[0:length]
    for offset in range(1, tap_count):
        running = running + tap_weights[offset] * padded[offset:offset + length]
    return running

def reference(tokens, input_norm_scale, outer_gate_weight, inner_gate_weight, value_weight_matrix, output_gate_weight, state_input_weight, write_key_weight, read_key_weight, step_size_weight, gated_conv_weight, input_conv_weight, write_conv_weight, read_conv_weight, step_size_bias, log_decay_rate, decay_spikes, direct_path_weight, head_norm_scale, conv_output_weight, state_output_weight):
    token_rows = tokens.astype(jnp.float32)
    scaled = token_rows * lax.rsqrt(lax.optimization_barrier(jnp.mean(token_rows * token_rows, axis=1, keepdims=True)) + epsilon)
    normed = (scaled * input_norm_scale.astype(jnp.float32)).astype(jnp.bfloat16)

    def project(weight):
        return jnp.dot(normed, weight, preferred_element_type=jnp.float32).astype(jnp.bfloat16)
    outer_gate = project(outer_gate_weight)
    inner_gate = project(inner_gate_weight)
    conv_input = project(value_weight_matrix)
    out_gate = project(output_gate_weight)
    state_input = project(state_input_weight)
    write_keys = project(write_key_weight)
    read_keys = project(read_key_weight)
    step_raw = jnp.dot(normed, step_size_weight, preferred_element_type=jnp.float32)
    product = inner_gate.astype(jnp.float32) * conv_input.astype(jnp.float32)
    mixer_part = (outer_gate.astype(jnp.float32) * causal_taps(product, gated_conv_weight.astype(jnp.float32))).astype(jnp.bfloat16)
    seq_input = jax.nn.silu(causal_taps(state_input.astype(jnp.float32), input_conv_weight.astype(jnp.float32)))
    seq_write = jax.nn.silu(causal_taps(write_keys.astype(jnp.float32), write_conv_weight.astype(jnp.float32)))
    seq_read = jax.nn.silu(causal_taps(read_keys.astype(jnp.float32), read_conv_weight.astype(jnp.float32)))
    discrete_step = jax.nn.softplus(step_raw + step_size_bias[None, :])
    step_logarithm = discrete_step * (-jnp.exp(log_decay_rate))[None, :] + decay_spikes.T
    blocks = SEQUENCE_TOKENS // BLOCK
    per_group = MIXER_HEADS // GROUPS
    input_blocks = seq_input.reshape(blocks, BLOCK, MIXER_HEADS, HEAD_DIM)
    weighted = input_blocks * discrete_step.reshape(blocks, BLOCK, MIXER_HEADS, 1)
    write_blocks = seq_write.reshape(blocks, BLOCK, GROUPS, STATE)
    read_blocks = seq_read.reshape(blocks, BLOCK, GROUPS, STATE)
    cumulative = jnp.cumsum(step_logarithm.reshape(blocks, BLOCK, MIXER_HEADS), axis=1)
    causal = lax.broadcasted_iota(jnp.int32, (BLOCK, BLOCK), 0) >= lax.broadcasted_iota(jnp.int32, (BLOCK, BLOCK), 1)

    def one_block(carried_state, inputs):
        block_weighted, block_write, block_read, block_cum = inputs
        write_heads = jnp.repeat(block_write, per_group, axis=1)
        read_heads = jnp.repeat(block_read, per_group, axis=1)
        scores = jnp.einsum('lhm,shm->lsh', read_heads, write_heads, precision=highest)
        damping = jnp.exp(jnp.where(causal[:, :, None], block_cum[:, None, :] - block_cum[None, :, :], -jnp.inf))
        within = jnp.einsum('lsh,shp->lhp', scores * damping, block_weighted, precision=highest)
        from_before = jnp.einsum('lhm,hpm->lhp', read_heads, carried_state, precision=highest) * jnp.exp(block_cum)[:, :, None]
        to_end = jnp.exp(block_cum[-1:, :] - block_cum)
        new_state = jnp.einsum('shm,shp->hpm', write_heads * to_end[:, :, None], block_weighted, precision=highest)
        return (carried_state * jnp.exp(block_cum[-1])[:, None, None] + new_state, within + from_before)
    _, block_outputs = lax.scan(one_block, jnp.zeros((MIXER_HEADS, HEAD_DIM, STATE), jnp.float32), (weighted, write_blocks, read_blocks, cumulative))
    head_out = block_outputs + direct_path_weight[None, None, :, None] * input_blocks
    head_out = head_out.reshape(SEQUENCE_TOKENS, MIXER_HEADS * HEAD_DIM)
    gated_heads = (head_out * jax.nn.silu(out_gate.astype(jnp.float32))).reshape(SEQUENCE_TOKENS, MIXER_HEADS, HEAD_DIM)
    normalized = gated_heads * lax.rsqrt(lax.optimization_barrier(jnp.mean(gated_heads * gated_heads, axis=2, keepdims=True)) + epsilon)
    state_part = (normalized.reshape(SEQUENCE_TOKENS, MIXER_HEADS * HEAD_DIM) * head_norm_scale.astype(jnp.float32)).astype(jnp.bfloat16)
    share_conv = CONV // N_TP
    share_state = MIXER_HEADS * HEAD_DIM // N_TP
    running = jnp.zeros((SEQUENCE_TOKENS, D), jnp.float32)
    for head_block in range(N_TP):
        conv_slice = slice(head_block * share_conv, (head_block + 1) * share_conv)
        state_slice = slice(head_block * share_state, (head_block + 1) * share_state)
        partial_sum = jnp.dot(mixer_part[:, conv_slice], conv_output_weight[conv_slice], preferred_element_type=jnp.float32)
        partial_sum = partial_sum + jnp.dot(state_part[:, state_slice], state_output_weight[state_slice], preferred_element_type=jnp.float32)
        rounded = lax.optimization_barrier(partial_sum.astype(jnp.bfloat16))
        running = running + rounded.astype(jnp.float32)
    return running.astype(jnp.bfloat16)
```

```python
import jax
import jax.numpy as jnp
from jax import lax
from jax.experimental import pallas as pl
from jax.experimental.pallas import tpu as pltpu
from jax.sharding import Mesh
from jax.sharding import PartitionSpec as P

SP = ("z", "x", "c")
SP_TP = ("z", "x", "c", "tp")
EPS = 1e-05
ROWS = 512
HALO = 16
BLK = 128
NB = ROWS // BLK
F32 = jnp.float32
BF16 = jnp.bfloat16


def call(body, outs, args, specs=None, scratch=()):
    vmem = pl.BlockSpec(memory_space=pltpu.VMEM)
    specs = specs or {}
    return pl.pallas_call(
        body,
        out_shape=outs,
        in_specs=[specs.get(i, vmem) for i in range(len(args))],
        out_specs=jax.tree.map(lambda _: vmem, outs),
        scratch_shapes=list(scratch),
    )(*args)


HBM = pl.BlockSpec(memory_space=pltpu.HBM)
SMEM = pl.BlockSpec(memory_space=pltpu.SMEM)


def shape(dims, kind):
    return jax.ShapeDtypeStruct(dims, kind)


def dot(a, b):
    return jnp.dot(a, b, preferred_element_type=F32)


def dot_nt(a, b):
    return lax.dot_general(a, b, (((1,), (1,)), ((), ())), preferred_element_type=F32)


def per_head(v):
    rows = v.shape[0]
    low = lax.broadcasted_iota(jnp.int32, (rows, 128), 1) < 64
    pairs = [
        jnp.where(
            low,
            jnp.broadcast_to(v[:, 2 * p : 2 * p + 1], (rows, 128)),
            jnp.broadcast_to(v[:, 2 * p + 1 : 2 * p + 2], (rows, 128)),
        )
        for p in range(2)
    ]
    return jnp.concatenate(pairs, axis=1)


def silu(v):
    return v / (1.0 + jnp.exp(-v))


def assemble(c, own, other, whole, sems, wait):
    for x in range(4):
        for side, src in ((0, own), (1, other)):
            at = c if side == 0 else 1 - c
            copy = pltpu.make_async_copy(
                src.at[x], whole.at[:, x, at], sems.at[2 * x + side]
            )
            if wait:
                copy.wait()
            else:
                copy.start()


def taps(ref, weights, cols, count):
    w = weights[...].astype(F32)
    out = None
    for k in range(count):
        part = w[k : k + 1, :] * ref[pl.ds(HALO - count + 1 + k, ROWS), cols]
        out = part if out is None else out + part
    return out


def norm_body(tok, halo, gain, ws, bias, rate, spikes, normed, dt, cum, cum_t):
    g = gain[...].astype(F32)

    def rows_of(v):
        f = v.astype(F32)
        scaled = f * lax.rsqrt(jnp.mean(f * f, axis=1, keepdims=True) + EPS)
        return (scaled * g).astype(BF16)

    normed[0:HALO, :] = rows_of(halo[...])
    for y in range(4):

        def some(i, _, y=y):
            at = pl.multiple_of(i * 16, 16)
            to = pl.multiple_of(HALO + y * 128 + i * 16, 16)
            normed[pl.ds(to, 16), :] = rows_of(tok[y, pl.ds(at, 16), :])
            return 0

        lax.fori_loop(0, 8, some, 0, unroll=2)
    raw = dot(normed[HALO:, :], ws[...]) + bias[...]
    step = jnp.maximum(raw, 0.0) + jnp.log1p(jnp.exp(-jnp.abs(raw)))
    dt[...] = step
    logs = -step * jnp.exp(rate[...]) + spikes[...]
    r = lax.broadcasted_iota(jnp.int32, (BLK, BLK), 0)
    s = lax.broadcasted_iota(jnp.int32, (BLK, BLK), 1)
    lower = jnp.where(r >= s, 1.0, 0.0).astype(F32)
    carry = jnp.zeros((1, 128), F32)
    for b in range(NB):
        part = (
            jnp.dot(
                lower,
                logs[b * BLK : (b + 1) * BLK],
                precision=lax.Precision.HIGHEST,
                preferred_element_type=F32,
            )
            + carry
        )
        cum[b * BLK : (b + 1) * BLK, :] = part
        cum_t[:, b * BLK : (b + 1) * BLK] = part.T[0:8, :]
        carry = part[BLK - 1 : BLK, :]


def first_body(
    c_ref, normed, own, other, dt, cum, input_taps, write_taps,
    weighted, seq_input, seq_write, local, pieces,
    whole, fields, sems,
):
    c = c_ref[0]
    assemble(c, own, other, whole, sems, False)
    assemble(c, own, other, whole, sems, True)
    projected = dot(normed[...], whole[...].reshape(2048, 384))
    fields[...] = projected.astype(BF16).astype(F32)
    xin = silu(taps(fields, input_taps, slice(0, 256), 4))
    write = silu(taps(fields, write_taps, slice(256, 384), 4))
    seq_input[...] = xin
    seq_write[...] = write.astype(BF16)
    scaled = xin * per_head(dt[:, 0:128])
    weighted[...] = scaled.astype(BF16)
    state = jnp.zeros((128, 256), F32)
    before = jnp.zeros((1, 128), F32)
    for b in range(NB):
        rows = slice(b * BLK, (b + 1) * BLK)
        end = cum[(b + 1) * BLK - 1 : (b + 1) * BLK, :]
        local[b] = state.astype(BF16)
        to_end = per_head(jnp.exp(end - cum[rows, :]))
        added = dot(write[rows].T.astype(BF16), (scaled[rows] * to_end).astype(BF16))
        state = state * per_head(jnp.exp(end - before)) + added
        before = end
    decay = per_head(jnp.exp(before))
    high = decay.astype(BF16).astype(F32)
    low = decay - high
    tail = jnp.where(
        lax.broadcasted_iota(jnp.int32, (8, 256), 0) < 4,
        jnp.broadcast_to(high, (8, 256)),
        jnp.broadcast_to(low, (8, 256)),
    ).astype(BF16)
    for j in range(8):
        pieces[j, 0:16, :] = state[16 * j : 16 * (j + 1)].astype(BF16)
        pieces[j, 16:24, :] = tail


def piece_of(ref, j):
    v = ref[j].astype(F32)
    return v[0:16], v[16:17] + v[20:21]


def plane_body(got, send):
    state = jnp.zeros((16, 256), F32)
    decay = jnp.ones((1, 256), F32)
    for j in range(8):
        s, d = piece_of(got, j)
        state = state * d + s
        decay = decay * d
    high = decay.astype(BF16).astype(F32)
    tail = jnp.where(
        lax.broadcasted_iota(jnp.int32, (8, 256), 0) < 4,
        jnp.broadcast_to(high, (8, 256)),
        jnp.broadcast_to(decay - high, (8, 256)),
    )
    one = jnp.concatenate([state, tail], axis=0).astype(BF16)
    for k in range(16):
        send[k] = one


def enter_body(z_ref, got, planes, out):
    z = z_ref[0]
    state = jnp.zeros((16, 256), F32)
    for k in range(16):
        s, d = piece_of(planes, k)
        state = jnp.where(k < z, state * d + s, state)
    for j in range(8):
        out[j] = state.astype(BF16)
        s, d = piece_of(got, j)
        state = state * d + s


def rest_body(
    c_ref, normed, own, other, weighted, seq_input, seq_write, local, cum, cum_t,
    read_taps, gated_taps, direct,
    partly, read_out, gate, mixer,
    whole, fields, sems,
):
    c = c_ref[0]
    assemble(c, own, other, whole, sems, False)
    assemble(c, own, other, whole, sems, True)
    n = normed[...]

    def projected(lo, hi):
        w = whole[:, :, :, :, lo:hi].reshape(2048, hi - lo)
        return dot(n, w).astype(BF16).astype(F32)

    fields[:, 0:128] = projected(0, 128)
    read = silu(taps(fields, read_taps, slice(0, 128), 4)).astype(BF16)
    read_out[...] = read
    gate[...] = silu(projected(128, 384)[HALO:])
    inner = projected(640, 896)
    fields[...] = inner * projected(896, 1152)
    outer = projected(384, 640)[HALO:]
    mixer[...] = (outer * taps(fields, gated_taps, slice(0, 256), 3)).astype(BF16)
    r = lax.broadcasted_iota(jnp.int32, (BLK, BLK), 0)
    s = lax.broadcasted_iota(jnp.int32, (BLK, BLK), 1)
    causal = r >= s
    low = s < 64
    before = jnp.zeros((1, 128), F32)
    for b in range(NB):
        rows = slice(b * BLK, (b + 1) * BLK)
        rb = read[rows]
        scores = dot_nt(rb, seq_write[rows, :])
        here = cum[rows, :]
        from_local = dot(rb, local[b]) * per_head(jnp.exp(here - before))
        before = here[BLK - 1 : BLK, :]
        halves = []
        for p in range(2):
            pair = weighted[rows, 128 * p : 128 * (p + 1)]
            two = []
            for h in (2 * p, 2 * p + 1):
                gap = here[:, h : h + 1] - cum_t[h : h + 1, rows]
                damped = scores * jnp.exp(jnp.where(causal, gap, -jnp.inf))
                two.append(dot(damped.astype(BF16), pair))
            halves.append(jnp.where(low, two[0], two[1]))
        within = jnp.concatenate(halves, axis=1)
        partly[rows, :] = within + from_local + direct[...] * seq_input[rows, :]


def tail_body(
    c_ref, arriving, partly, read, gate, cum, mixer, scale, own, other,
    out,
    whole, act, sems,
):
    c = c_ref[0]
    assemble(c, own, other, whole, sems, False)
    act[:, 0:256] = mixer[...]
    head = partly[...] + dot(read[...], arriving[...]) * per_head(jnp.exp(cum[...]))
    gated = head * gate[...]
    square = gated * gated
    r = lax.broadcasted_iota(jnp.int32, (256, 256), 0) // 64
    s = lax.broadcasted_iota(jnp.int32, (256, 256), 1) // 64
    same = jnp.where(r == s, 1.0 / 64.0, 0.0).astype(BF16)
    high = square.astype(BF16)
    rest = (square - high.astype(F32)).astype(BF16)
    mean = dot(high, same) + dot(rest, same)
    act[:, 256:512] = (gated * lax.rsqrt(mean + EPS) * scale[...].astype(F32)).astype(BF16)
    assemble(c, own, other, whole, sems, True)
    w = whole[...].reshape(2048, 512)
    a = act[...]
    for q in range(4):
        cols = slice(512 * q, 512 * (q + 1))
        out[:, cols] = dot_nt(a, w[cols]).astype(BF16)


def sum_body(got, out):
    v = got[0].astype(F32)
    for y in range(1, 4):
        v = v + got[y].astype(F32)
    out[...] = v.astype(BF16)


def copies(shard, axis):
    n = lax.axis_size(axis)
    return lax.all_to_all(
        jnp.broadcast_to(shard[None], (n, *shard.shape)), axis, 0, 0, tiled=True
    )


def swapped(shard):
    return lax.ppermute(shard, "c", [(0, 1), (1, 0)])


def lanes(v, width=128):
    return jnp.pad(v, ((0, 0), (0, width - v.shape[1])))


def per_device(
    tokens,
    input_norm_scale,
    outer_gate_weight,
    inner_gate_weight,
    value_weight_matrix,
    output_gate_weight,
    state_input_weight,
    write_key_weight,
    read_key_weight,
    step_size_weight,
    gated_conv_weight,
    input_conv_weight,
    write_conv_weight,
    read_conv_weight,
    step_size_bias,
    log_decay_rate,
    decay_spikes,
    direct_path_weight,
    head_norm_scale,
    conv_output_weight,
    state_output_weight,
):
    c = lax.axis_index("c").astype(jnp.int32).reshape(1)
    z = lax.axis_index("z").astype(jnp.int32).reshape(1)
    tok = copies(tokens, "tp")
    own_in = jnp.concatenate(
        [
            state_input_weight,
            write_key_weight,
            read_key_weight,
            output_gate_weight,
            outer_gate_weight,
            inner_gate_weight,
            value_weight_matrix,
        ],
        axis=1,
    )
    column = lax.all_gather(own_in, "z", axis=0, tiled=False)
    first = copies(column[:, :, :384], "x")
    first_other = swapped(first)
    rest = copies(column[:, :, 384:], "x")
    rest_other = swapped(rest)
    own_out = jnp.concatenate([conv_output_weight, state_output_weight], axis=0).T
    wide = copies(copies(own_out, "z"), "x")
    wide_other = swapped(wide)
    steps = 128
    halo = lax.ppermute(tok[3, 112:, :], SP, [(i, i + 1) for i in range(steps - 1)])

    normed, dt, cum, cum_t = call(
        norm_body,
        (
            shape((HALO + ROWS, 2048), BF16),
            shape((ROWS, 128), F32),
            shape((ROWS, 128), F32),
            shape((8, ROWS), F32),
        ),
        (
            tok,
            halo,
            input_norm_scale[None],
            lanes(step_size_weight),
            lanes(step_size_bias[None]),
            lanes(log_decay_rate[None]),
            lanes(decay_spikes.T),
        ),
    )
    weighted, seq_input, seq_write, local, pieces = call(
        first_body,
        (
            shape((ROWS, 256), BF16),
            shape((ROWS, 256), F32),
            shape((ROWS, 128), BF16),
            shape((NB, 128, 256), BF16),
            shape((8, 24, 256), BF16),
        ),
        (c, normed, first, first_other, dt, cum, input_conv_weight, write_conv_weight),
        {0: SMEM, 2: HBM, 3: HBM},
        (
            pltpu.VMEM((16, 4, 2, 16, 384), BF16),
            pltpu.VMEM((HALO + ROWS, 384), F32),
            pltpu.SemaphoreType.DMA((8,)),
        ),
    )
    got = lax.all_to_all(pieces, ("x", "c"), 0, 0, tiled=True)
    planes = lax.all_to_all(
        call(plane_body, shape((16, 24, 256), BF16), (got,)), "z", 0, 0, tiled=True
    )
    entering = call(enter_body, shape((8, 16, 256), BF16), (z, got, planes), {0: SMEM})
    arriving = lax.all_to_all(entering, ("x", "c"), 0, 0, tiled=True).reshape(128, 256)

    direct = jnp.repeat(direct_path_weight, 64)[None]
    partly, read, gate, mixer = call(
        rest_body,
        (
            shape((ROWS, 256), F32),
            shape((ROWS, 128), BF16),
            shape((ROWS, 256), F32),
            shape((ROWS, 256), BF16),
        ),
        (
            c, normed, rest, rest_other, weighted, seq_input, seq_write, local, cum, cum_t,
            read_conv_weight, gated_conv_weight, direct,
        ),
        {0: SMEM, 2: HBM, 3: HBM},
        (
            pltpu.VMEM((16, 4, 2, 16, 1152), BF16),
            pltpu.VMEM((HALO + ROWS, 256), F32),
            pltpu.SemaphoreType.DMA((8,)),
        ),
    )
    partial = call(
        tail_body,
        shape((ROWS, 2048), BF16),
        (c, arriving, partly, read, gate, cum, mixer, head_norm_scale[None], wide, wide_other),
        {0: SMEM, 8: HBM, 9: HBM},
        (
            pltpu.VMEM((16, 4, 2, 16, 512), BF16),
            pltpu.VMEM((ROWS, 512), BF16),
            pltpu.SemaphoreType.DMA((8,)),
        ),
    )
    parts = lax.all_to_all(partial.reshape(4, 128, 2048), "tp", 0, 0, tiled=True)
    return call(sum_body, shape((128, 2048), BF16), (parts,))


def solution(mesh):
    torus = Mesh(mesh.devices.reshape(16, 4, 2, mesh.shape["tp"]), SP_TP)
    rows = P(SP, "tp")
    cols = P("tp", SP)
    taps_ = P(None, "tp")
    heads = P("tp")
    return jax.shard_map(
        per_device,
        mesh=torus,
        in_specs=(
            P(SP_TP, None), P(), rows, rows, rows, rows, rows, rows, rows,
            taps_, taps_, taps_, taps_, taps_, heads, heads, cols, heads, heads, cols, cols,
        ),
        out_specs=P(SP_TP, None),
        check_vma=False,
    )
```

```python
import jax
import jax.numpy as jnp
from jax import lax
from jax.experimental import pallas as pl
from jax.experimental.pallas import tpu as pltpu
from jax.sharding import Mesh
from jax.sharding import PartitionSpec as P

SP = ("z", "x", "c")
SP_TP = ("z", "x", "c", "tp")
EPS = 1e-05
ROWS = 512
HALO = 16
BLK = 128
NB = ROWS // BLK
F32 = jnp.float32
BF16 = jnp.bfloat16


def call(body, outs, args, specs=None, scratch=()):
    vmem = pl.BlockSpec(memory_space=pltpu.VMEM)
    specs = specs or {}
    return pl.pallas_call(
        body,
        out_shape=outs,
        in_specs=[specs.get(i, vmem) for i in range(len(args))],
        out_specs=jax.tree.map(lambda _: vmem, outs),
        scratch_shapes=list(scratch),
    )(*args)


HBM = pl.BlockSpec(memory_space=pltpu.HBM)
SMEM = pl.BlockSpec(memory_space=pltpu.SMEM)


def shape(dims, kind):
    return jax.ShapeDtypeStruct(dims, kind)


def dot(a, b):
    return jnp.dot(a, b, preferred_element_type=F32)


def dot_nt(a, b):
    return lax.dot_general(a, b, (((1,), (1,)), ((), ())), preferred_element_type=F32)


def per_head(v):
    rows = v.shape[0]
    low = lax.broadcasted_iota(jnp.int32, (rows, 128), 1) < 64
    pairs = [
        jnp.where(
            low,
            jnp.broadcast_to(v[:, 2 * p : 2 * p + 1], (rows, 128)),
            jnp.broadcast_to(v[:, 2 * p + 1 : 2 * p + 2], (rows, 128)),
        )
        for p in range(2)
    ]
    return jnp.concatenate(pairs, axis=1)


def silu(v):
    return v / (1.0 + jnp.exp(-v))


def run(copies, wait):
    for copy in copies:
        if wait:
            copy.wait()
        else:
            copy.start()


def first_copies(c, own, other, whole, sems):
    return [
        pltpu.make_async_copy(
            src.at[x], whole.at[:, x, c if side == 0 else 1 - c], sems.at[2 * x + side]
        )
        for x in range(4)
        for side, src in ((0, own), (1, other))
    ]


def ring_copies(x, c, parts, whole, sems, lo, count):
    out = []
    for side in range(2):
        at = c if side == 0 else 1 - c
        for i, (by, z, zs) in enumerate(
            ((0, 0, 16), (3, 0, 16), (1, 0, 16), (2, 0, 8), (2, 8, 8))
        ):
            out.append(
                pltpu.make_async_copy(
                    parts[5 * side + i].at[:, lo : lo + count, :],
                    whole.at[z : z + zs, (x + by) % 4, at],
                    sems.at[5 * side + i],
                )
            )
    return out


def block(whole, q):
    return whole[:, :, :, 16 * q : 16 * (q + 1), :].reshape(2048, 128)


def blocks(whole, lo, count):
    return jnp.concatenate([block(whole, q) for q in range(lo, lo + count)], axis=1)


def taps(ref, weights, cols, count):
    w = weights[...].astype(F32)
    out = None
    for k in range(count):
        part = w[k : k + 1, :] * ref[pl.ds(HALO - count + 1 + k, ROWS), cols]
        out = part if out is None else out + part
    return out


def prep_body(tok, gain, w0, w1, w2, w3, w4, w5, w6, w7, w8, copied, own, left):
    q = 0
    for w in (w0, w1, w2, w3, w4, w5, w6, w7, w8):
        for k in range(w.shape[1] // 128):
            v = w[:, 128 * k : 128 * (k + 1)]
            if q < 15:
                own[16 * q : 16 * (q + 1), :] = v
            else:
                own[240:254, :] = v[0:14]
                f = v.astype(F32)
                left[...] = jnp.concatenate([f[14:15], f[15:16]], axis=1)
            q += 1
    g = gain[...].astype(F32)

    def some(i, _):
        rows = pl.ds(pl.multiple_of(i * 16, 16), 16)
        f = tok[rows, :].astype(F32)
        scaled = f * lax.rsqrt(jnp.mean(f * f, axis=1, keepdims=True) + EPS)
        v = (scaled * g).astype(BF16)
        for y in range(4):
            copied[y, rows, :] = v
        return 0

    lax.fori_loop(0, 8, some, 0, unroll=2)


def cum_body(tok, ws, params, spikes, dt, cum, cum_t):
    n = tok[...].reshape(ROWS, 2048)
    raw = dot_nt(ws[...], n)[0:8] + params[0:8, 0:1]
    step = jnp.maximum(raw, 0.0) + jnp.log1p(jnp.exp(-jnp.abs(raw)))
    logs = -step * jnp.exp(params[0:8, 1:2]) + spikes[...]
    r = lax.broadcasted_iota(jnp.int32, (BLK, BLK), 0)
    s = lax.broadcasted_iota(jnp.int32, (BLK, BLK), 1)
    upper = jnp.where(r <= s, 1.0, 0.0).astype(F32)
    carry = jnp.zeros((8, 1), F32)
    fill = jnp.zeros((BLK - 8, BLK), F32)
    for b in range(NB):
        rows = slice(b * BLK, (b + 1) * BLK)
        part = (
            jnp.dot(
                logs[:, rows],
                upper,
                precision=lax.Precision.HIGHEST,
                preferred_element_type=F32,
            )
            + carry
        )
        cum_t[:, rows] = part
        cum[rows, :] = jnp.concatenate([part, fill], axis=0).T
        dt[rows, :] = jnp.concatenate([step[:, rows], fill], axis=0).T
        carry = part[:, BLK - 1 : BLK]


def first_body(
    pos, tok, halo, own, other, dt, cum, input_taps, write_taps,
    weighted, seq_input, seq_write, local, pieces,
    whole, normed, fields, sems,
):
    moves = first_copies(pos[2], own, other, whole, sems)
    run(moves, False)
    normed[0:HALO, :] = halo[...]
    normed[HALO:, :] = tok[...].reshape(ROWS, 2048)
    run(moves, True)
    projected = dot(normed[...], blocks(whole, 0, 3))
    fields[...] = projected.astype(BF16).astype(F32)
    xin = silu(taps(fields, input_taps, slice(0, 256), 4))
    write = silu(taps(fields, write_taps, slice(256, 384), 4))
    seq_input[...] = xin
    seq_write[...] = write.astype(BF16)
    scaled = xin * per_head(dt[:, 0:128])
    weighted[...] = scaled.astype(BF16)
    state = jnp.zeros((128, 256), F32)
    before = jnp.zeros((1, 128), F32)
    for b in range(NB):
        rows = slice(b * BLK, (b + 1) * BLK)
        end = cum[(b + 1) * BLK - 1 : (b + 1) * BLK, :]
        local[b] = state.astype(BF16)
        to_end = per_head(jnp.exp(end - cum[rows, :]))
        added = dot(write[rows].T.astype(BF16), (scaled[rows] * to_end).astype(BF16))
        state = state * per_head(jnp.exp(end - before)) + added
        before = end
    decay = per_head(jnp.exp(before))
    high = decay.astype(BF16).astype(F32)
    low = decay - high
    tail = jnp.where(
        lax.broadcasted_iota(jnp.int32, (8, 256), 0) < 4,
        jnp.broadcast_to(high, (8, 256)),
        jnp.broadcast_to(low, (8, 256)),
    ).astype(BF16)
    for j in range(8):
        pieces[j, 0:16, :] = state[16 * j : 16 * (j + 1)].astype(BF16)
        pieces[j, 16:24, :] = tail


def piece_of(ref, j):
    v = ref[j].astype(F32)
    return v[0:16], v[16:17] + v[20:21]


def plane_body(got, left, send):
    state = jnp.zeros((16, 256), F32)
    decay = jnp.ones((1, 256), F32)
    for j in range(8):
        s, d = piece_of(got, j)
        state = state * d + s
        decay = decay * d
    high = decay.astype(BF16).astype(F32)
    tail = jnp.where(
        lax.broadcasted_iota(jnp.int32, (8, 256), 0) < 4,
        jnp.broadcast_to(high, (8, 256)),
        jnp.broadcast_to(decay - high, (8, 256)),
    )
    second = lax.broadcasted_iota(jnp.int32, (8, 256), 0) == 1
    tail = jnp.where(second, jnp.broadcast_to(left[...], (8, 256)), tail)
    one = jnp.concatenate([state, tail], axis=0).astype(BF16)
    for k in range(16):
        send[k] = one


def enter_body(pos, got, planes, out):
    z = pos[0]
    state = jnp.zeros((16, 256), F32)
    lefts = []
    for k in range(16):
        lefts.append(planes[k].astype(F32)[17:18])
        s, d = piece_of(planes, k)
        state = jnp.where(k < z, state * d + s, state)
    left = jnp.concatenate(lefts, axis=0).astype(BF16)
    for j in range(8):
        out[j, 0:16, :] = state.astype(BF16)
        out[j, 16:32, :] = left
        s, d = piece_of(got, j)
        state = state * d + s


def rest_body(
    pos, tok, halo, p0, p1, p2, p3, p4, p5, p6, p7, p8, p9,
    weighted, seq_input, seq_write, local, cum, cum_t,
    read_taps, gated_taps, direct,
    partly, read_out, gate, mixer,
    whole, normed, fields, sems,
):
    parts = (p0, p1, p2, p3, p4, p5, p6, p7, p8, p9)
    moves = ring_copies(pos[1], pos[2], parts, whole, sems, 0, 144)
    run(moves, False)
    normed[0:HALO, :] = halo[...]
    normed[HALO:, :] = tok[...].reshape(ROWS, 2048)
    run(moves, True)
    n = normed[...]

    def projected(lo, count):
        return dot(n, blocks(whole, lo, count)).astype(BF16).astype(F32)

    fields[:, 0:128] = projected(0, 1)
    read = silu(taps(fields, read_taps, slice(0, 128), 4)).astype(BF16)
    read_out[...] = read
    gate[...] = silu(projected(1, 2)[HALO:])
    inner = projected(5, 2)
    fields[...] = inner * projected(7, 2)
    outer = projected(3, 2)[HALO:]
    mixer[...] = (outer * taps(fields, gated_taps, slice(0, 256), 3)).astype(BF16)
    r = lax.broadcasted_iota(jnp.int32, (BLK, BLK), 0)
    s = lax.broadcasted_iota(jnp.int32, (BLK, BLK), 1)
    causal = r >= s
    low = s < 64
    before = jnp.zeros((1, 128), F32)
    for b in range(NB):
        rows = slice(b * BLK, (b + 1) * BLK)
        rb = read[rows]
        scores = dot_nt(rb, seq_write[rows, :])
        here = cum[rows, :]
        from_local = dot(rb, local[b]) * per_head(jnp.exp(here - before))
        before = here[BLK - 1 : BLK, :]
        halves = []
        for p in range(2):
            pair = weighted[rows, 128 * p : 128 * (p + 1)]
            two = []
            for h in (2 * p, 2 * p + 1):
                gap = here[:, h : h + 1] - cum_t[h : h + 1, rows]
                damped = scores * jnp.exp(jnp.where(causal, gap, -jnp.inf))
                two.append(dot(damped.astype(BF16), pair))
            halves.append(jnp.where(low, two[0], two[1]))
        within = jnp.concatenate(halves, axis=1)
        partly[rows, :] = within + from_local + direct[...] * seq_input[rows, :]


def tail_body(
    pos, arriving, partly, read, gate, cum, mixer, scale,
    p0, p1, p2, p3, p4, p5, p6, p7, p8, p9,
    out,
    whole, act, sems,
):
    parts = (p0, p1, p2, p3, p4, p5, p6, p7, p8, p9)
    moves = ring_copies(pos[1], pos[2], parts, whole, sems, 144, 64)
    run(moves, False)
    act[:, 0:256] = mixer[...]
    state = jnp.concatenate([arriving[j, 0:16, :] for j in range(8)], axis=0)
    head = partly[...] + dot(read[...], state) * per_head(jnp.exp(cum[...]))
    gated = head * gate[...]
    square = gated * gated
    r = lax.broadcasted_iota(jnp.int32, (256, 256), 0) // 64
    s = lax.broadcasted_iota(jnp.int32, (256, 256), 1) // 64
    same = jnp.where(r == s, 1.0 / 64.0, 0.0).astype(BF16)
    high = square.astype(BF16)
    rest = (square - high.astype(F32)).astype(BF16)
    mean = dot(high, same) + dot(rest, same)
    act[:, 256:512] = (gated * lax.rsqrt(mean + EPS) * scale[...].astype(F32)).astype(BF16)
    run(moves, True)
    row = lax.broadcasted_iota(jnp.int32, (16, 128), 0)
    for j in range(8):
        lefts = arriving[j, 16:32, :].astype(F32)
        for z in range(16):
            tile = whole[z, j // 2, j % 2, 48:64, :].astype(F32)
            for i in range(2):
                v = lefts[z : z + 1, 128 * i : 128 * (i + 1)]
                tile = jnp.where(row == 14 + i, jnp.broadcast_to(v, (16, 128)), tile)
            whole[z, j // 2, j % 2, 48:64, :] = tile.astype(BF16)
    a = act[...]
    for q in range(4):
        cols = slice(512 * q, 512 * (q + 1))
        some = whole.at[4 * q : 4 * (q + 1)]
        w = jnp.concatenate(
            [some[:, :, :, 16 * k : 16 * (k + 1), :].reshape(512, 128) for k in range(4)],
            axis=1,
        )
        out[:, cols] = dot_nt(a, w).astype(BF16)


def sum_body(got, out):
    v = got[0].astype(F32)
    for y in range(1, 4):
        v = v + got[y].astype(F32)
    out[...] = v.astype(BF16)


def exchanged(tiles, axis):
    return lax.all_to_all(tiles, axis, 0, 0, tiled=True)


def copies(shard, axis):
    n = lax.axis_size(axis)
    return exchanged(jnp.broadcast_to(shard[None], (n, *shard.shape)), axis)


def passed(shard, by):
    return lax.ppermute(shard, "x", [(i, (i + by) % 4) for i in range(4)])


def swapped(shard):
    return lax.ppermute(shard, "c", [(0, 1), (1, 0)])


def per_device(
    tokens,
    input_norm_scale,
    outer_gate_weight,
    inner_gate_weight,
    value_weight_matrix,
    output_gate_weight,
    state_input_weight,
    write_key_weight,
    read_key_weight,
    step_size_weight,
    gated_conv_weight,
    input_conv_weight,
    write_conv_weight,
    read_conv_weight,
    step_size_bias,
    log_decay_rate,
    decay_spikes,
    direct_path_weight,
    head_norm_scale,
    conv_output_weight,
    state_output_weight,
):
    pos = jnp.stack([lax.axis_index(a).astype(jnp.int32) for a in SP])
    copied, own, left = call(
        prep_body,
        (shape((4, 128, 2048), BF16), shape((254, 128), BF16), shape((1, 256), F32)),
        (
            tokens,
            input_norm_scale[None],
            state_input_weight,
            write_key_weight,
            read_key_weight,
            output_gate_weight,
            outer_gate_weight,
            inner_gate_weight,
            value_weight_matrix,
            conv_output_weight.T,
            state_output_weight.T,
        ),
    )
    tok = exchanged(copied, "tp")
    column = lax.all_gather(own, "z", axis=0, tiled=False)
    first = copies(column[:, :48], "x")
    first_other = swapped(first)
    ring = [jnp.pad(column[:, 48:], ((0, 0), (0, 2), (0, 0)))]
    ring.append(passed(ring[0], 1))
    ring.append(passed(ring[0], 3))
    ring.append(passed(ring[1][:8], 1))
    ring.append(passed(ring[2][8:], 3))
    ring += [swapped(part) for part in ring]
    halo = lax.ppermute(tok[3, 112:, :], SP, [(i, i + 1) for i in range(127)])

    dt, cum, cum_t = call(
        cum_body,
        (shape((ROWS, 128), F32), shape((ROWS, 128), F32), shape((8, ROWS), F32)),
        (
            tok,
            jnp.pad(step_size_weight.T, ((0, 12), (0, 0))),
            jnp.pad(jnp.stack([step_size_bias, log_decay_rate], 1), ((0, 4), (0, 126))),
            jnp.pad(decay_spikes, ((0, 4), (0, 0))),
        ),
    )
    weighted, seq_input, seq_write, local, pieces = call(
        first_body,
        (
            shape((ROWS, 256), BF16),
            shape((ROWS, 256), F32),
            shape((ROWS, 128), BF16),
            shape((NB, 128, 256), BF16),
            shape((8, 24, 256), BF16),
        ),
        (pos, tok, halo, first, first_other, dt, cum, input_conv_weight, write_conv_weight),
        {0: SMEM, 3: HBM, 4: HBM},
        (
            pltpu.VMEM((16, 4, 2, 48, 128), BF16),
            pltpu.VMEM((HALO + ROWS, 2048), BF16),
            pltpu.VMEM((HALO + ROWS, 384), F32),
            pltpu.SemaphoreType.DMA((8,)),
        ),
    )
    got = exchanged(pieces, ("x", "c"))
    send = call(plane_body, shape((16, 24, 256), BF16), (got, left))
    planes = exchanged(send, "z")
    entering = call(
        enter_body, shape((8, 32, 256), BF16), (pos, got, planes), {0: SMEM}
    )
    arriving = exchanged(entering, ("x", "c"))

    direct = jnp.repeat(direct_path_weight, 64)[None]
    partly, read, gate, mixer = call(
        rest_body,
        (
            shape((ROWS, 256), F32),
            shape((ROWS, 128), BF16),
            shape((ROWS, 256), F32),
            shape((ROWS, 256), BF16),
        ),
        (
            pos, tok, halo, *ring, weighted, seq_input, seq_write, local, cum, cum_t,
            read_conv_weight, gated_conv_weight, direct,
        ),
        {0: SMEM, **{i: HBM for i in range(3, 13)}},
        (
            pltpu.VMEM((16, 4, 2, 144, 128), BF16),
            pltpu.VMEM((HALO + ROWS, 2048), BF16),
            pltpu.VMEM((HALO + ROWS, 256), F32),
            pltpu.SemaphoreType.DMA((10,)),
        ),
    )
    partial = call(
        tail_body,
        shape((ROWS, 2048), BF16),
        (pos, arriving, partly, read, gate, cum, mixer, head_norm_scale[None], *ring),
        {0: SMEM, **{i: HBM for i in range(8, 18)}},
        (
            pltpu.VMEM((16, 4, 2, 64, 128), BF16),
            pltpu.VMEM((ROWS, 512), BF16),
            pltpu.SemaphoreType.DMA((10,)),
        ),
    )
    parts = exchanged(partial.reshape(4, 128, 2048), "tp")
    return call(sum_body, shape((128, 2048), BF16), (parts,))


def solution(mesh):
    torus = Mesh(mesh.devices.reshape(16, 4, 2, mesh.shape["tp"]), SP_TP)
    rows = P(SP, "tp")
    cols = P("tp", SP)
    taps_ = P(None, "tp")
    heads = P("tp")
    return jax.shard_map(
        per_device,
        mesh=torus,
        in_specs=(
            P(SP_TP, None), P(), rows, rows, rows, rows, rows, rows, rows,
            taps_, taps_, taps_, taps_, taps_, heads, heads, cols, heads, heads, cols, cols,
        ),
        out_specs=P(SP_TP, None),
        check_vma=False,
    )
```

```python
import jax
import jax.numpy as jnp
from jax import lax
from jax.experimental import pallas as pl
from jax.experimental.pallas import tpu as pltpu
from jax.sharding import Mesh
from jax.sharding import PartitionSpec as P

SP = ("z", "x", "c")
SP_TP = ("z", "x", "c", "tp")
EPS = 1e-05
ROWS = 512
HALO = 16
BLK = 128
NB = ROWS // BLK
F32 = jnp.float32
BF16 = jnp.bfloat16


def call(body, outs, args, specs=None, scratch=()):
    vmem = pl.BlockSpec(memory_space=pltpu.VMEM)
    specs = specs or {}
    return pl.pallas_call(
        body,
        out_shape=outs,
        in_specs=[specs.get(i, vmem) for i in range(len(args))],
        out_specs=jax.tree.map(lambda _: vmem, outs),
        scratch_shapes=list(scratch),
    )(*args)


HBM = pl.BlockSpec(memory_space=pltpu.HBM)
SMEM = pl.BlockSpec(memory_space=pltpu.SMEM)


def shape(dims, kind):
    return jax.ShapeDtypeStruct(dims, kind)


def dot(a, b):
    return jnp.dot(a, b, preferred_element_type=F32)


def dot_nt(a, b):
    return lax.dot_general(a, b, (((1,), (1,)), ((), ())), preferred_element_type=F32)


def per_head(v):
    rows = v.shape[0]
    low = lax.broadcasted_iota(jnp.int32, (rows, 128), 1) < 64
    pairs = [
        jnp.where(
            low,
            jnp.broadcast_to(v[:, 2 * p : 2 * p + 1], (rows, 128)),
            jnp.broadcast_to(v[:, 2 * p + 1 : 2 * p + 2], (rows, 128)),
        )
        for p in range(2)
    ]
    return jnp.concatenate(pairs, axis=1)


def silu(v):
    return v / (1.0 + jnp.exp(-v))


def run(copies, wait):
    for copy in copies:
        if wait:
            copy.wait()
        else:
            copy.start()


def first_copies(own, other, whole, sems):
    c = lax.axis_index("c")
    return [
        pltpu.make_async_copy(
            src.at[x], whole.at[:, x, c if side == 0 else 1 - c], sems.at[2 * x + side]
        )
        for x in range(4)
        for side, src in ((0, own), (1, other))
    ]


def ring_copies(parts, whole, sems, lo, count):
    x, c = lax.axis_index("x"), lax.axis_index("c")
    out = []
    for side in range(2):
        at = c if side == 0 else 1 - c
        for i, by in enumerate((0, 3 - 2 * at, 1 + 2 * at, 2)):
            out.append(
                pltpu.make_async_copy(
                    parts[4 * side + i].at[:, lo : lo + count, :],
                    whole.at[:, (x + by) % 4, at],
                    sems.at[4 * side + i],
                )
            )
    return out


def block(whole, q):
    return whole[:, :, :, 16 * q : 16 * (q + 1), :].reshape(2048, 128)


def blocks(whole, lo, count):
    return jnp.concatenate([block(whole, q) for q in range(lo, lo + count)], axis=1)


def taps(ref, weights, cols, count):
    w = weights[...].astype(F32)
    out = None
    for k in range(count):
        part = w[k : k + 1, :] * ref[pl.ds(HALO - count + 1 + k, ROWS), cols]
        out = part if out is None else out + part
    return out


def prep_body(tok, gain, w0, w1, w2, w3, w4, w5, w6, w7, w8, copied, own, left):
    q = 0
    for w in (w0, w1, w2, w3, w4, w5, w6, w7, w8):
        for k in range(w.shape[1] // 128):
            v = w[:, 128 * k : 128 * (k + 1)]
            if q < 15:
                own[16 * q : 16 * (q + 1), :] = v
            else:
                own[240:254, :] = v[0:14]
                f = v.astype(F32)
                left[...] = jnp.concatenate([f[14:15], f[15:16]], axis=1)
            q += 1
    g = gain[...].astype(F32)

    def some(i, _):
        rows = pl.ds(pl.multiple_of(i * 16, 16), 16)
        f = tok[rows, :].astype(F32)
        scaled = f * lax.rsqrt(jnp.mean(f * f, axis=1, keepdims=True) + EPS)
        v = (scaled * g).astype(BF16)
        for y in range(4):
            copied[y, rows, :] = v
        return 0

    lax.fori_loop(0, 8, some, 0, unroll=2)


def cum_body(tok, ws, bias, rate, spikes, dt, cum, cum_t, square):
    n = tok[...].reshape(ROWS, 2048)
    raw = dot_nt(ws[...], n) + bias[...]
    step = jnp.maximum(raw, 0.0) + jnp.log1p(jnp.exp(-jnp.abs(raw)))
    logs = -step * jnp.exp(rate[...]) + spikes[...]
    r = lax.broadcasted_iota(jnp.int32, (BLK, BLK), 0)
    s = lax.broadcasted_iota(jnp.int32, (BLK, BLK), 1)
    upper = jnp.where(r <= s, 1.0, 0.0).astype(F32)
    carry = jnp.zeros((4, 1), F32)
    square[...] = jnp.zeros(square.shape, F32)
    for b in range(NB):
        rows = slice(b * BLK, (b + 1) * BLK)
        part = (
            jnp.dot(
                logs[:, rows],
                upper,
                precision=lax.Precision.HIGHEST,
                preferred_element_type=F32,
            )
            + carry
        )
        cum_t[0:4, rows] = part
        square[0, 0:4, :] = part
        square[1, 0:4, :] = step[:, rows]
        cum[rows, :] = square[0].T
        dt[rows, :] = square[1].T
        carry = part[:, BLK - 1 : BLK]


def first_body(
    tok, halo, own, other, dt, cum, input_taps, write_taps,
    weighted, seq_input, seq_write, local, pieces,
    whole, normed, fields, sems,
):
    moves = first_copies(own, other, whole, sems)
    run(moves, False)
    normed[0:HALO, :] = halo[...]
    normed[HALO:, :] = tok[...].reshape(ROWS, 2048)
    run(moves, True)
    projected = dot(normed[...], blocks(whole, 0, 3))
    fields[...] = projected.astype(BF16).astype(F32)
    xin = silu(taps(fields, input_taps, slice(0, 256), 4))
    write = silu(taps(fields, write_taps, slice(256, 384), 4))
    seq_input[...] = xin
    seq_write[...] = write.astype(BF16)
    scaled = xin * per_head(dt[:, 0:128])
    weighted[...] = scaled.astype(BF16)
    state = jnp.zeros((128, 256), F32)
    before = jnp.zeros((1, 128), F32)
    for b in range(NB):
        rows = slice(b * BLK, (b + 1) * BLK)
        end = cum[(b + 1) * BLK - 1 : (b + 1) * BLK, :]
        local[b] = state.astype(BF16)
        to_end = per_head(jnp.exp(end - cum[rows, :]))
        added = dot(write[rows].T.astype(BF16), (scaled[rows] * to_end).astype(BF16))
        state = state * per_head(jnp.exp(end - before)) + added
        before = end
    decay = per_head(jnp.exp(before))
    high = decay.astype(BF16).astype(F32)
    low = decay - high
    tail = jnp.where(
        lax.broadcasted_iota(jnp.int32, (8, 256), 0) < 4,
        jnp.broadcast_to(high, (8, 256)),
        jnp.broadcast_to(low, (8, 256)),
    ).astype(BF16)
    for j in range(8):
        pieces[j, 0:16, :] = state[16 * j : 16 * (j + 1)].astype(BF16)
        pieces[j, 16:24, :] = tail


def piece_of(ref, j):
    v = ref[j].astype(F32)
    return v[0:16], v[16:17] + v[20:21]


def plane_body(got, left, send):
    state = jnp.zeros((16, 256), F32)
    decay = jnp.ones((1, 256), F32)
    for j in range(8):
        s, d = piece_of(got, j)
        state = state * d + s
        decay = decay * d
    high = decay.astype(BF16).astype(F32)
    tail = jnp.where(
        lax.broadcasted_iota(jnp.int32, (8, 256), 0) < 4,
        jnp.broadcast_to(high, (8, 256)),
        jnp.broadcast_to(decay - high, (8, 256)),
    )
    second = lax.broadcasted_iota(jnp.int32, (8, 256), 0) == 1
    tail = jnp.where(second, jnp.broadcast_to(left[...], (8, 256)), tail)
    one = jnp.concatenate([state, tail], axis=0).astype(BF16)
    for k in range(16):
        send[k] = one


def enter_body(got, planes, out):
    z = lax.axis_index("z")
    state = jnp.zeros((16, 256), F32)
    lefts = []
    for k in range(16):
        lefts.append(planes[k].astype(F32)[17:18])
        s, d = piece_of(planes, k)
        state = jnp.where(k < z, state * d + s, state)
    left = jnp.concatenate(lefts, axis=0).astype(BF16)
    for j in range(8):
        out[j, 0:16, :] = state.astype(BF16)
        out[j, 16:32, :] = left
        s, d = piece_of(got, j)
        state = state * d + s


def rest_body(
    tok, halo, p0, p1, p2, p3, p4, p5, p6, p7, read_taps, gated_taps,
    read_out, gate, mixer,
    whole, normed, fields, sems,
):
    parts = (p0, p1, p2, p3, p4, p5, p6, p7)
    moves = ring_copies(parts, whole, sems, 0, 144)
    run(moves, False)
    normed[0:HALO, :] = halo[...]
    normed[HALO:, :] = tok[...].reshape(ROWS, 2048)
    run(moves, True)
    n = normed[...]

    def projected(lo, count):
        return dot(n, blocks(whole, lo, count)).astype(BF16).astype(F32)

    fields[:, 0:128] = projected(0, 1)
    read_out[...] = silu(taps(fields, read_taps, slice(0, 128), 4)).astype(BF16)
    gate[...] = silu(projected(1, 2)[HALO:])
    inner = projected(5, 2)
    fields[...] = inner * projected(7, 2)
    outer = projected(3, 2)[HALO:]
    mixer[...] = (outer * taps(fields, gated_taps, slice(0, 256), 3)).astype(BF16)


def within_body(
    read, weighted, seq_input, seq_write, local, cum, cum_t, direct, partly
):
    weight = per_head(direct[...])
    r = lax.broadcasted_iota(jnp.int32, (BLK, BLK), 0)
    s = lax.broadcasted_iota(jnp.int32, (BLK, BLK), 1)
    causal = r >= s
    low = s < 64
    before = jnp.zeros((1, 128), F32)
    for b in range(NB):
        rows = slice(b * BLK, (b + 1) * BLK)
        rb = read[rows, :]
        scores = dot_nt(rb, seq_write[rows, :])
        here = cum[rows, :]
        from_local = dot(rb, local[b]) * per_head(jnp.exp(here - before))
        before = here[BLK - 1 : BLK, :]
        halves = []
        for p in range(2):
            pair = weighted[rows, 128 * p : 128 * (p + 1)]
            two = []
            for h in (2 * p, 2 * p + 1):
                gap = here[:, h : h + 1] - cum_t[h : h + 1, rows]
                damped = scores * jnp.exp(jnp.where(causal, gap, -jnp.inf))
                two.append(dot(damped.astype(BF16), pair))
            halves.append(jnp.where(low, two[0], two[1]))
        within = jnp.concatenate(halves, axis=1)
        partly[rows, :] = within + from_local + weight * seq_input[rows, :]


def wide_weights(parts, arriving, whole, sems):
    moves = ring_copies(parts, whole, sems, 144, 64)
    run(moves, False)

    def finish():
        run(moves, True)
        row = lax.broadcasted_iota(jnp.int32, (16, 128), 0)
        for j in range(8):
            lefts = arriving[j, 16:32, :].astype(F32)
            for z in range(16):
                tile = whole[z, j // 2, j % 2, 48:64, :].astype(F32)
                for i in range(2):
                    v = lefts[z : z + 1, 128 * i : 128 * (i + 1)]
                    v = jnp.broadcast_to(v, (16, 128))
                    tile = jnp.where(row == 14 + i, v, tile)
                whole[z, j // 2, j % 2, 48:64, :] = tile.astype(BF16)

    return finish


def project_out(act, at, whole, out):
    a = act[pl.ds(pl.multiple_of(at * 128, 128), 128), :]
    for q in range(4):
        some = whole.at[4 * q : 4 * (q + 1)]
        w = jnp.concatenate(
            [some[:, :, :, 16 * k : 16 * (k + 1), :].reshape(512, 128) for k in range(4)],
            axis=1,
        )
        out[:, 512 * q : 512 * (q + 1)] = dot_nt(a, w).astype(out.dtype)


def tail_body(
    arriving, partly, read, gate, cum, mixer, scale,
    p0, p1, p2, p3, p4, p5, p6, p7,
    act, far, beside,
    whole, sems,
):
    finish = wide_weights((p0, p1, p2, p3, p4, p5, p6, p7), arriving, whole, sems)
    act[:, 0:256] = mixer[...]
    state = jnp.concatenate([arriving[j, 0:16, :] for j in range(8)], axis=0)
    head = partly[...] + dot(read[...], state) * per_head(jnp.exp(cum[...]))
    gated = head * gate[...]
    square = gated * gated
    r = lax.broadcasted_iota(jnp.int32, (256, 256), 0) // 64
    s = lax.broadcasted_iota(jnp.int32, (256, 256), 1) // 64
    same = jnp.where(r == s, 1.0 / 64.0, 0.0).astype(BF16)
    high = square.astype(BF16)
    rest = (square - high.astype(F32)).astype(BF16)
    mean = dot(high, same) + dot(rest, same)
    act[:, 256:512] = (gated * lax.rsqrt(mean + EPS) * scale[...].astype(F32)).astype(BF16)
    finish()
    y, c = lax.axis_index("tp"), lax.axis_index("c")
    project_out(act, (y + 2) % 4, whole, far)
    project_out(act, (y + 3 + 2 * c) % 4, whole, beside)


def near_body(
    arriving, act, p0, p1, p2, p3, p4, p5, p6, p7, near, mine, whole, sems
):
    wide_weights((p0, p1, p2, p3, p4, p5, p6, p7), arriving, whole, sems)()
    y, c = lax.axis_index("tp"), lax.axis_index("c")
    project_out(act, (y + 1 + 2 * c) % 4, whole, near)
    project_out(act, y, whole, mine)


def add_body(near, got, out):
    out[...] = (near[...] + got[...].astype(F32)).astype(BF16)


def sum_body(mine, a, b, out):
    out[...] = (mine[...] + a[...].astype(F32) + b[...].astype(F32)).astype(BF16)


def exchanged(tiles, axis):
    return lax.all_to_all(tiles, axis, 0, 0, tiled=True)


def copies(shard, axis):
    n = lax.axis_size(axis)
    return exchanged(jnp.broadcast_to(shard[None], (n, *shard.shape)), axis)


def two_way(shard, axis, toward):
    steps = [(i, c, (i + (toward if c == 0 else -toward)) % 4) for i in range(4) for c in range(2)]
    if axis == "x":
        return lax.ppermute(shard, ("x", "c"), [(2 * i + c, 2 * j + c) for i, c, j in steps])
    return lax.ppermute(shard, ("c", "tp"), [(4 * c + i, 4 * c + j) for i, c, j in steps])


def swapped(shard):
    return lax.ppermute(shard, "c", [(0, 1), (1, 0)])


def per_device(
    tokens,
    input_norm_scale,
    outer_gate_weight,
    inner_gate_weight,
    value_weight_matrix,
    output_gate_weight,
    state_input_weight,
    write_key_weight,
    read_key_weight,
    step_size_weight,
    gated_conv_weight,
    input_conv_weight,
    write_conv_weight,
    read_conv_weight,
    step_size_bias,
    log_decay_rate,
    decay_spikes,
    direct_path_weight,
    head_norm_scale,
    conv_output_weight,
    state_output_weight,
):
    copied, own, left = call(
        prep_body,
        (shape((4, 128, 2048), BF16), shape((254, 128), BF16), shape((1, 256), F32)),
        (
            tokens,
            input_norm_scale[None],
            state_input_weight,
            write_key_weight,
            read_key_weight,
            output_gate_weight,
            outer_gate_weight,
            inner_gate_weight,
            value_weight_matrix,
            conv_output_weight.T,
            state_output_weight.T,
        ),
    )
    tok = exchanged(copied, "tp")
    column = lax.all_gather(own, "z", axis=0, tiled=False)
    first = copies(column[:, :48], "x")
    first_other = swapped(first)
    ring = [jnp.pad(column[:, 48:], ((0, 0), (0, 2), (0, 0)))]
    ring.append(two_way(ring[0], "x", 1))
    ring.append(two_way(ring[0], "x", -1))
    ring.append(two_way(ring[1], "x", 1))
    ring += [swapped(part) for part in ring]
    halo = lax.ppermute(tok[3, 112:, :], SP, [(i, i + 1) for i in range(127)])

    dt, cum, cum_t = call(
        cum_body,
        (shape((ROWS, 128), F32), shape((ROWS, 128), F32), shape((8, ROWS), F32)),
        (
            tok,
            step_size_weight.T,
            step_size_bias[:, None],
            log_decay_rate[:, None],
            decay_spikes,
        ),
        scratch=(pltpu.VMEM((2, BLK, BLK), F32),),
    )
    weighted, seq_input, seq_write, local, pieces = call(
        first_body,
        (
            shape((ROWS, 256), BF16),
            shape((ROWS, 256), F32),
            shape((ROWS, 128), BF16),
            shape((NB, 128, 256), BF16),
            shape((8, 24, 256), BF16),
        ),
        (tok, halo, first, first_other, dt, cum, input_conv_weight, write_conv_weight),
        {2: HBM, 3: HBM},
        (
            pltpu.VMEM((16, 4, 2, 48, 128), BF16),
            pltpu.VMEM((HALO + ROWS, 2048), BF16),
            pltpu.VMEM((HALO + ROWS, 384), F32),
            pltpu.SemaphoreType.DMA((8,)),
        ),
    )
    got = exchanged(pieces, ("x", "c"))
    send = call(plane_body, shape((16, 24, 256), BF16), (got, left))
    planes = exchanged(send, "z")
    entering = call(enter_body, shape((8, 32, 256), BF16), (got, planes))
    arriving = exchanged(entering, ("x", "c"))

    read, gate, mixer = call(
        rest_body,
        (
            shape((ROWS, 128), BF16),
            shape((ROWS, 256), F32),
            shape((ROWS, 256), BF16),
        ),
        (tok, halo, *ring, read_conv_weight, gated_conv_weight),
        {i: HBM for i in range(2, 10)},
        (
            pltpu.VMEM((16, 4, 2, 144, 128), BF16),
            pltpu.VMEM((HALO + ROWS, 2048), BF16),
            pltpu.VMEM((HALO + ROWS, 256), F32),
            pltpu.SemaphoreType.DMA((8,)),
        ),
    )
    partly = call(
        within_body,
        shape((ROWS, 256), F32),
        (read, weighted, seq_input, seq_write, local, cum, cum_t, direct_path_weight[None]),
    )
    wide = (pltpu.VMEM((16, 4, 2, 64, 128), BF16), pltpu.SemaphoreType.DMA((8,)))
    act, far, beside = call(
        tail_body,
        (shape((ROWS, 512), BF16), shape((128, 2048), BF16), shape((128, 2048), BF16)),
        (arriving, partly, read, gate, cum, mixer, head_norm_scale[None], *ring),
        {i: HBM for i in range(7, 15)},
        wide,
    )
    got_far = two_way(far, "tp", 1)
    got_beside = two_way(beside, "tp", -1)
    near, mine = call(
        near_body,
        (shape((128, 2048), F32), shape((128, 2048), F32)),
        (arriving, act, *ring),
        {i: HBM for i in range(2, 10)},
        wide,
    )
    both = call(add_body, shape((128, 2048), BF16), (near, got_far))
    got_near = two_way(both, "tp", 1)
    return call(sum_body, shape((128, 2048), BF16), (mine, got_beside, got_near))


def solution(mesh):
    torus = Mesh(mesh.devices.reshape(16, 4, 2, mesh.shape["tp"]), SP_TP)
    rows = P(SP, "tp")
    cols = P("tp", SP)
    taps_ = P(None, "tp")
    heads = P("tp")
    return jax.shard_map(
        per_device,
        mesh=torus,
        in_specs=(
            P(SP_TP, None), P(), rows, rows, rows, rows, rows, rows, rows,
            taps_, taps_, taps_, taps_, taps_, heads, heads, cols, heads, heads, cols, cols,
        ),
        out_specs=P(SP_TP, None),
        check_vma=False,
    )
```

```python
import jax
import jax.numpy as jnp
from jax import lax
from jax.experimental import pallas as pl
from jax.experimental.pallas import tpu as pltpu
from jax.sharding import Mesh
from jax.sharding import PartitionSpec as P

SP = ("z", "x", "c")
SP_TP = ("z", "x", "c", "tp")
EPS = 1e-05
ROWS = 512
HALO = 16
BLK = 128
NB = ROWS // BLK
F32 = jnp.float32
BF16 = jnp.bfloat16


def call(body, outs, args, scratch=(), mib=8):
    vmem = pl.BlockSpec(memory_space=pltpu.VMEM)
    return pl.pallas_call(
        body,
        out_shape=outs,
        in_specs=[vmem for _ in args],
        out_specs=jax.tree.map(lambda _: vmem, outs),
        scratch_shapes=list(scratch),
        compiler_params=pltpu.CompilerParams(vmem_limit_bytes=mib * 2**20),
    )(*args)


def shape(dims, kind):
    return jax.ShapeDtypeStruct(dims, kind)


def dot(a, b):
    return jnp.dot(a, b, preferred_element_type=F32)


def dot_nt(a, b):
    return lax.dot_general(a, b, (((1,), (1,)), ((), ())), preferred_element_type=F32)


def per_head(v):
    rows = v.shape[0]
    low = lax.broadcasted_iota(jnp.int32, (rows, 128), 1) < 64
    pairs = [
        jnp.where(
            low,
            jnp.broadcast_to(v[:, 2 * p : 2 * p + 1], (rows, 128)),
            jnp.broadcast_to(v[:, 2 * p + 1 : 2 * p + 2], (rows, 128)),
        )
        for p in range(2)
    ]
    return jnp.concatenate(pairs, axis=1)


def silu(v):
    return v / (1.0 + jnp.exp(-v))


def lay_out(pieces, targets):
    def some(z, _):
        for get, x, c in pieces:
            for ref, lo, count in targets:
                ref[z, x, c] = get(z, lo, count)
        return 0

    lax.fori_loop(0, 16, some, 0)


def first_pieces(own, other):
    c = lax.axis_index("c")
    return [
        (lambda z, lo, n, r=ref, x=x: r[x, z, lo : lo + n, :], x, at)
        for ref, at in ((own, c), (other, 1 - c))
        for x in range(4)
    ]


def ring_pieces(parts):
    x, c = lax.axis_index("x"), lax.axis_index("c")
    return [
        (
            lambda z, lo, n, r=parts[4 * side + i]: r[z, lo : lo + n, :],
            (x + by) % 4,
            at,
        )
        for side, at in ((0, c), (1, 1 - c))
        for i, by in enumerate((0, 3 - 2 * at, 1 + 2 * at, 2))
    ]


def block(whole, q):
    return whole[:, :, :, 16 * q : 16 * (q + 1), :].reshape(2048, 128)


def blocks(whole, lo, count):
    return jnp.concatenate([block(whole, q) for q in range(lo, lo + count)], axis=1)


def taps(ref, weights, cols, count):
    w = weights[...].astype(F32)
    out = None
    for k in range(count):
        part = w[k : k + 1, :] * ref[pl.ds(HALO - count + 1 + k, ROWS), cols]
        out = part if out is None else out + part
    return out


def prep_body(tok, gain, w0, w1, w2, w3, w4, w5, w6, w7, w8, copied, own, left):
    q = 0
    for w in (w0, w1, w2, w3, w4, w5, w6, w7, w8):
        for k in range(w.shape[1] // 128):
            v = w[:, 128 * k : 128 * (k + 1)]
            if q < 15:
                own[16 * q : 16 * (q + 1), :] = v
            else:
                own[240:254, :] = v[0:14]
                f = v.astype(F32)
                left[...] = jnp.concatenate([f[14:15], f[15:16]], axis=1)
            q += 1
    g = gain[...].astype(F32)

    def some(i, _):
        rows = pl.ds(pl.multiple_of(i * 16, 16), 16)
        f = tok[rows, :].astype(F32)
        scaled = f * lax.rsqrt(jnp.mean(f * f, axis=1, keepdims=True) + EPS)
        v = (scaled * g).astype(BF16)
        for y in range(4):
            copied[y, rows, :] = v
        return 0

    lax.fori_loop(0, 8, some, 0, unroll=2)


def cum_body(tok, ws, bias, rate, spikes, dt, cum, cum_t, square):
    n = tok[...].reshape(ROWS, 2048)
    raw = dot_nt(ws[...], n) + bias[...]
    step = jnp.maximum(raw, 0.0) + jnp.log1p(jnp.exp(-jnp.abs(raw)))
    logs = -step * jnp.exp(rate[...]) + spikes[...]
    r = lax.broadcasted_iota(jnp.int32, (BLK, BLK), 0)
    s = lax.broadcasted_iota(jnp.int32, (BLK, BLK), 1)
    upper = jnp.where(r <= s, 1.0, 0.0).astype(F32)
    carry = jnp.zeros((4, 1), F32)
    square[...] = jnp.zeros(square.shape, F32)
    for b in range(NB):
        rows = slice(b * BLK, (b + 1) * BLK)
        part = (
            jnp.dot(
                logs[:, rows],
                upper,
                precision=lax.Precision.HIGHEST,
                preferred_element_type=F32,
            )
            + carry
        )
        cum_t[0:4, rows] = part
        square[0, 0:4, :] = part
        square[1, 0:4, :] = step[:, rows]
        cum[rows, :] = square[0].T
        dt[rows, :] = square[1].T
        carry = part[:, BLK - 1 : BLK]


def first_body(
    tok, halo, own, other, dt, cum, input_taps, write_taps,
    weighted, seq_input, seq_write, local, pieces,
    whole, normed, fields,
):
    lay_out(first_pieces(own, other), ((whole, 0, 48),))
    normed[0:HALO, :] = halo[...]
    normed[HALO:, :] = tok[...].reshape(ROWS, 2048)
    projected = dot(normed[...], blocks(whole, 0, 3))
    fields[...] = projected.astype(BF16).astype(F32)
    xin = silu(taps(fields, input_taps, slice(0, 256), 4))
    write = silu(taps(fields, write_taps, slice(256, 384), 4))
    seq_input[...] = xin
    seq_write[...] = write.astype(BF16)
    scaled = xin * per_head(dt[:, 0:128])
    weighted[...] = scaled.astype(BF16)
    state = jnp.zeros((128, 256), F32)
    before = jnp.zeros((1, 128), F32)
    for b in range(NB):
        rows = slice(b * BLK, (b + 1) * BLK)
        end = cum[(b + 1) * BLK - 1 : (b + 1) * BLK, :]
        local[b] = state.astype(BF16)
        to_end = per_head(jnp.exp(end - cum[rows, :]))
        added = dot(write[rows].T.astype(BF16), (scaled[rows] * to_end).astype(BF16))
        state = state * per_head(jnp.exp(end - before)) + added
        before = end
    decay = per_head(jnp.exp(before))
    high = decay.astype(BF16).astype(F32)
    low = decay - high
    tail = jnp.where(
        lax.broadcasted_iota(jnp.int32, (8, 256), 0) < 4,
        jnp.broadcast_to(high, (8, 256)),
        jnp.broadcast_to(low, (8, 256)),
    ).astype(BF16)
    for j in range(8):
        pieces[j, 0:16, :] = state[16 * j : 16 * (j + 1)].astype(BF16)
        pieces[j, 16:24, :] = tail


def piece_of(ref, j):
    v = ref[j].astype(F32)
    return v[0:16], v[16:17] + v[20:21]


def plane_body(got, left, send):
    state = jnp.zeros((16, 256), F32)
    decay = jnp.ones((1, 256), F32)
    for j in range(8):
        s, d = piece_of(got, j)
        state = state * d + s
        decay = decay * d
    high = decay.astype(BF16).astype(F32)
    tail = jnp.where(
        lax.broadcasted_iota(jnp.int32, (8, 256), 0) < 4,
        jnp.broadcast_to(high, (8, 256)),
        jnp.broadcast_to(decay - high, (8, 256)),
    )
    second = lax.broadcasted_iota(jnp.int32, (8, 256), 0) == 1
    tail = jnp.where(second, jnp.broadcast_to(left[...], (8, 256)), tail)
    one = jnp.concatenate([state, tail], axis=0).astype(BF16)
    for k in range(16):
        send[k] = one


def enter_body(got, planes, out):
    z = lax.axis_index("z")
    state = jnp.zeros((16, 256), F32)
    lefts = []
    for k in range(16):
        lefts.append(planes[k].astype(F32)[17:18])
        s, d = piece_of(planes, k)
        state = jnp.where(k < z, state * d + s, state)
    left = jnp.concatenate(lefts, axis=0).astype(BF16)
    for j in range(8):
        out[j, 0:16, :] = state.astype(BF16)
        out[j, 16:32, :] = left
        s, d = piece_of(got, j)
        state = state * d + s


def rest_body(
    tok, halo, p0, p1, p2, p3, p4, p5, p6, p7, read_taps, gated_taps,
    read_out, gate, mixer, wide,
    whole, normed, fields,
):
    parts = ring_pieces((p0, p1, p2, p3, p4, p5, p6, p7))
    lay_out(parts, ((whole, 0, 144), (wide, 144, 64)))
    normed[0:HALO, :] = halo[...]
    normed[HALO:, :] = tok[...].reshape(ROWS, 2048)
    n = normed[...]

    def projected(lo, count):
        return dot(n, blocks(whole, lo, count)).astype(BF16).astype(F32)

    fields[:, 0:128] = projected(0, 1)
    read_out[...] = silu(taps(fields, read_taps, slice(0, 128), 4)).astype(BF16)
    gate[...] = silu(projected(1, 2)[HALO:])
    inner = projected(5, 2)
    fields[...] = inner * projected(7, 2)
    outer = projected(3, 2)[HALO:]
    mixer[...] = (outer * taps(fields, gated_taps, slice(0, 256), 3)).astype(BF16)


def within_body(
    read, weighted, seq_input, seq_write, local, cum, cum_t, direct, partly
):
    weight = per_head(direct[...])
    r = lax.broadcasted_iota(jnp.int32, (BLK, BLK), 0)
    s = lax.broadcasted_iota(jnp.int32, (BLK, BLK), 1)
    causal = r >= s
    low = s < 64
    before = jnp.zeros((1, 128), F32)
    for b in range(NB):
        rows = slice(b * BLK, (b + 1) * BLK)
        rb = read[rows, :]
        scores = dot_nt(rb, seq_write[rows, :])
        here = cum[rows, :]
        from_local = dot(rb, local[b]) * per_head(jnp.exp(here - before))
        before = here[BLK - 1 : BLK, :]
        halves = []
        for p in range(2):
            pair = weighted[rows, 128 * p : 128 * (p + 1)]
            two = []
            for h in (2 * p, 2 * p + 1):
                gap = here[:, h : h + 1] - cum_t[h : h + 1, rows]
                damped = scores * jnp.exp(jnp.where(causal, gap, -jnp.inf))
                two.append(dot(damped.astype(BF16), pair))
            halves.append(jnp.where(low, two[0], two[1]))
        within = jnp.concatenate(halves, axis=1)
        partly[rows, :] = within + from_local + weight * seq_input[rows, :]


def patch(wide, arriving, fixed):
    row = lax.broadcasted_iota(jnp.int32, (16, 128), 0)
    for j in range(8):
        lefts = arriving[j, 16:32, :].astype(F32)
        for z in range(16):
            tile = wide[z, j // 2, j % 2, 48:64, :].astype(F32)
            for i in range(2):
                v = lefts[z : z + 1, 128 * i : 128 * (i + 1)]
                tile = jnp.where(row == 14 + i, jnp.broadcast_to(v, (16, 128)), tile)
            fixed[z, j // 2, j % 2] = tile.astype(BF16)


def project_out(act, at, wide, fixed, out):
    a = act[pl.ds(pl.multiple_of(at * 128, 128), 128), :]
    for q in range(4):
        zs = slice(4 * q, 4 * (q + 1))
        w = [wide[zs, :, :, 16 * k : 16 * (k + 1), :].reshape(512, 128) for k in range(3)]
        w = jnp.concatenate([*w, fixed[zs].reshape(512, 128)], axis=1)
        out[:, 512 * q : 512 * (q + 1)] = dot_nt(a, w).astype(out.dtype)


def tail_body(
    arriving, partly, read, gate, cum, mixer, scale, wide, act, far, fixed
):
    act[:, 0:256] = mixer[...]
    state = jnp.concatenate([arriving[j, 0:16, :] for j in range(8)], axis=0)
    head = partly[...] + dot(read[...], state) * per_head(jnp.exp(cum[...]))
    gated = head * gate[...]
    square = gated * gated
    r = lax.broadcasted_iota(jnp.int32, (256, 256), 0) // 64
    s = lax.broadcasted_iota(jnp.int32, (256, 256), 1) // 64
    same = jnp.where(r == s, 1.0 / 64.0, 0.0).astype(BF16)
    high = square.astype(BF16)
    rest = (square - high.astype(F32)).astype(BF16)
    mean = dot(high, same) + dot(rest, same)
    act[:, 256:512] = (gated * lax.rsqrt(mean + EPS) * scale[...].astype(F32)).astype(BF16)
    patch(wide, arriving, fixed)
    project_out(act, (lax.axis_index("tp") + 2) % 4, wide, fixed, far)


def near_body(act, wide, fixed, beside, near, mine):
    y, c = lax.axis_index("tp"), lax.axis_index("c")
    project_out(act, (y + 3 + 2 * c) % 4, wide, fixed, beside)
    project_out(act, (y + 1 + 2 * c) % 4, wide, fixed, near)
    project_out(act, y, wide, fixed, mine)


def add_body(near, got, out):
    out[...] = (near[...].astype(F32) + got[...].astype(F32)).astype(BF16)


def sum_body(mine, a, b, out):
    v = mine[...].astype(F32) + a[...].astype(F32)
    out[...] = (v + b[...].astype(F32)).astype(BF16)


def exchanged(tiles, axis):
    return lax.all_to_all(tiles, axis, 0, 0, tiled=True)


def copies(shard, axis):
    n = lax.axis_size(axis)
    return exchanged(jnp.broadcast_to(shard[None], (n, *shard.shape)), axis)


def two_way(shard, axis, toward):
    steps = [(i, c, (i + (toward if c == 0 else -toward)) % 4) for i in range(4) for c in range(2)]
    if axis == "x":
        return lax.ppermute(shard, ("x", "c"), [(2 * i + c, 2 * j + c) for i, c, j in steps])
    return lax.ppermute(shard, ("c", "tp"), [(4 * c + i, 4 * c + j) for i, c, j in steps])


def swapped(shard):
    return lax.ppermute(shard, "c", [(0, 1), (1, 0)])


def per_device(
    tokens,
    input_norm_scale,
    outer_gate_weight,
    inner_gate_weight,
    value_weight_matrix,
    output_gate_weight,
    state_input_weight,
    write_key_weight,
    read_key_weight,
    step_size_weight,
    gated_conv_weight,
    input_conv_weight,
    write_conv_weight,
    read_conv_weight,
    step_size_bias,
    log_decay_rate,
    decay_spikes,
    direct_path_weight,
    head_norm_scale,
    conv_output_weight,
    state_output_weight,
):
    copied, own, left = call(
        prep_body,
        (shape((4, 128, 2048), BF16), shape((254, 128), BF16), shape((1, 256), F32)),
        (
            tokens,
            input_norm_scale[None],
            state_input_weight,
            write_key_weight,
            read_key_weight,
            output_gate_weight,
            outer_gate_weight,
            inner_gate_weight,
            value_weight_matrix,
            conv_output_weight.T,
            state_output_weight.T,
        ),
    )
    tok = exchanged(copied, "tp")
    column = lax.all_gather(own, "z", axis=0, tiled=False)
    first = copies(column[:, :48], "x")
    first_other = swapped(first)
    ring = [jnp.pad(column[:, 48:], ((0, 0), (0, 2), (0, 0)))]
    ring.append(two_way(ring[0], "x", 1))
    ring.append(two_way(ring[0], "x", -1))
    ring.append(two_way(ring[1], "x", 1))
    ring += [swapped(part) for part in ring]
    halo = lax.ppermute(tok[3, 112:, :], SP, [(i, i + 1) for i in range(127)])

    dt, cum, cum_t = call(
        cum_body,
        (shape((ROWS, 128), F32), shape((ROWS, 128), F32), shape((8, ROWS), F32)),
        (
            tok,
            step_size_weight.T,
            step_size_bias[:, None],
            log_decay_rate[:, None],
            decay_spikes,
        ),
        scratch=(pltpu.VMEM((2, BLK, BLK), F32),),
    )
    weighted, seq_input, seq_write, local, pieces = call(
        first_body,
        (
            shape((ROWS, 256), BF16),
            shape((ROWS, 256), F32),
            shape((ROWS, 128), BF16),
            shape((NB, 128, 256), BF16),
            shape((8, 24, 256), BF16),
        ),
        (tok, halo, first, first_other, dt, cum, input_conv_weight, write_conv_weight),
        (
            pltpu.VMEM((16, 4, 2, 48, 128), BF16),
            pltpu.VMEM((HALO + ROWS, 2048), BF16),
            pltpu.VMEM((HALO + ROWS, 384), F32),
        ),
        mib=16,
    )
    got = exchanged(pieces, ("x", "c"))
    send = call(plane_body, shape((16, 24, 256), BF16), (got, left))
    planes = exchanged(send, "z")
    entering = call(enter_body, shape((8, 32, 256), BF16), (got, planes))
    arriving = exchanged(entering, ("x", "c"))

    read, gate, mixer, wide = call(
        rest_body,
        (
            shape((ROWS, 128), BF16),
            shape((ROWS, 256), F32),
            shape((ROWS, 256), BF16),
            shape((16, 4, 2, 64, 128), BF16),
        ),
        (tok, halo, *ring, read_conv_weight, gated_conv_weight),
        scratch=(
            pltpu.VMEM((16, 4, 2, 144, 128), BF16),
            pltpu.VMEM((HALO + ROWS, 2048), BF16),
            pltpu.VMEM((HALO + ROWS, 256), F32),
        ),
        mib=28,
    )
    partly = call(
        within_body,
        shape((ROWS, 256), F32),
        (read, weighted, seq_input, seq_write, local, cum, cum_t, direct_path_weight[None]),
    )
    act, far, fixed = call(
        tail_body,
        (
            shape((ROWS, 512), BF16),
            shape((128, 2048), BF16),
            shape((16, 4, 2, 16, 128), BF16),
        ),
        (arriving, partly, read, gate, cum, mixer, head_norm_scale[None], wide),
        mib=16,
    )
    got_far = two_way(far, "tp", 1)
    block_ = shape((128, 2048), BF16)
    beside, near, mine = call(
        near_body, (block_, block_, block_), (act, wide, fixed), mib=12
    )
    got_beside = two_way(beside, "tp", -1)
    both = call(add_body, shape((128, 2048), BF16), (near, got_far))
    got_near = two_way(both, "tp", 1)
    return call(sum_body, shape((128, 2048), BF16), (mine, got_beside, got_near))


def solution(mesh):
    torus = Mesh(mesh.devices.reshape(16, 4, 2, mesh.shape["tp"]), SP_TP)
    rows = P(SP, "tp")
    cols = P("tp", SP)
    taps_ = P(None, "tp")
    heads = P("tp")
    return jax.shard_map(
        per_device,
        mesh=torus,
        in_specs=(
            P(SP_TP, None), P(), rows, rows, rows, rows, rows, rows, rows,
            taps_, taps_, taps_, taps_, taps_, heads, heads, cols, heads, heads, cols, cols,
        ),
        out_specs=P(SP_TP, None),
        check_vma=False,
    )
```

```python
import jax
import jax.numpy as jnp
from jax import lax
from jax.experimental import pallas as pl
from jax.experimental.pallas import tpu as pltpu
from jax.sharding import Mesh
from jax.sharding import PartitionSpec as P

SP = ("z", "x", "c")
SP_TP = ("z", "x", "c", "tp")
EPS = 1e-05
ROWS = 512
HALO = 16
BLK = 128
NB = ROWS // BLK
F32 = jnp.float32
BF16 = jnp.bfloat16


def call(body, outs, args, scratch=(), mib=8, far_in=(), far_out=()):
    vmem = pl.BlockSpec(memory_space=pltpu.VMEM)
    hbm = pl.BlockSpec(memory_space=pltpu.HBM)
    many = isinstance(outs, tuple)
    args = [
        pltpu.with_memory_space_constraint(a, pltpu.HBM) if i in far_in else a
        for i, a in enumerate(args)
    ]
    return pl.pallas_call(
        body,
        out_shape=outs,
        in_specs=[hbm if i in far_in else vmem for i in range(len(args))],
        out_specs=tuple(hbm if i in far_out else vmem for i in range(len(outs))) if many else vmem,
        scratch_shapes=list(scratch),
        compiler_params=pltpu.CompilerParams(
            vmem_limit_bytes=None if mib is None else mib * 2**20
        ),
    )(*args)


def shape(dims, kind):
    return jax.ShapeDtypeStruct(dims, kind)


def on_chip(dims, kind):
    return pltpu.VMEM(dims, kind)


def main_memory(dims, kind):
    return pltpu.HBM(dims, kind)


def dot(a, b):
    return jnp.dot(a, b, preferred_element_type=F32)


def dot_nt(a, b):
    return lax.dot_general(a, b, (((1,), (1,)), ((), ())), preferred_element_type=F32)


def per_head(v):
    rows = v.shape[0]
    low = lax.broadcasted_iota(jnp.int32, (rows, 128), 1) < 64
    pairs = [
        jnp.where(
            low,
            jnp.broadcast_to(v[:, 2 * p : 2 * p + 1], (rows, 128)),
            jnp.broadcast_to(v[:, 2 * p + 1 : 2 * p + 2], (rows, 128)),
        )
        for p in range(2)
    ]
    return jnp.concatenate(pairs, axis=1)


def silu(v):
    return v / (1.0 + jnp.exp(-v))


def lay_out(pieces, targets):
    def some(z, _):
        for get, x, c in pieces:
            for ref, lo, count in targets:
                ref[z, x, c] = get(z, lo, count)
        return 0

    lax.fori_loop(0, 16, some, 0)


def first_pieces(own, other):
    c = lax.axis_index("c")
    return [
        (lambda z, lo, n, r=ref, x=x: r[x, z, lo : lo + n, :], x, at)
        for ref, at in ((own, c), (other, 1 - c))
        for x in range(4)
    ]


def ring_places():
    x, c = lax.axis_index("x"), lax.axis_index("c")
    return [
        ((x + by) % 4, at)
        for at in (c, 1 - c)
        for by in (0, 3 - 2 * at, 1 + 2 * at, 2)
    ]


def ring_copies(parts, which, target, lo, count, sems):
    places = ring_places()
    copies = []
    for i in which:
        x, at = places[i]
        copies.append(
            pltpu.make_async_copy(
                parts[i].at[:, lo : lo + count, :], target.at[:, x, at], sems.at[i]
            )
        )
    for copy in copies:
        copy.start()
    return copies


def ring_pieces(parts, which):
    places = ring_places()
    return [
        (lambda z, lo, n, r=parts[i]: r[z, lo : lo + n, :], *places[i]) for i in which
    ]


FAR = (0, 1, 2, 4)
NEAR = (3, 5, 6, 7)


def wait_for(copies):
    for copy in copies:
        copy.wait()


def block(whole, q):
    return whole[:, :, :, 16 * q : 16 * (q + 1), :].reshape(2048, 128)


def blocks(whole, lo, count):
    return jnp.concatenate([block(whole, q) for q in range(lo, lo + count)], axis=1)


def taps(ref, w, cols, count):
    out = None
    for k in range(count):
        part = w[k : k + 1, :] * ref[pl.ds(HALO - count + 1 + k, ROWS), cols]
        out = part if out is None else out + part
    return out


def prep_body(
    tok, gain, w0, w1, w2, w3, w4, w5, w6, w7, w8,
    gated_taps, input_taps, write_taps, read_taps, scale, direct, bias, rate,
    copied, own, left, small,
):
    q = 0
    for w in (w0, w1, w2, w3, w4, w5, w6, w7, w8):
        for k in range(w.shape[1] // 128):
            v = w[:, 128 * k : 128 * (k + 1)]
            if q < 15:
                own[16 * q : 16 * (q + 1), :] = v
            else:
                own[240:254, :] = v[0:14]
                f = v.astype(F32)
                left[...] = jnp.concatenate([f[14:15], f[15:16]], axis=1)
            q += 1
    small[...] = jnp.zeros(small.shape, F32)
    small[0:3, :] = gated_taps[...].astype(F32)
    small[3:7, :] = input_taps[...].astype(F32)
    small[7:11, 0:128] = write_taps[...].astype(F32)
    small[11:15, 0:128] = read_taps[...].astype(F32)
    f = scale[...].astype(F32)
    small[15:16, :] = jnp.concatenate([f[0:1], f[1:2]], axis=1)
    small[16:17, 0:4] = direct[...]
    small[17:18, 0:4] = bias[...]
    small[18:19, 0:4] = rate[...]
    f = gain[...].astype(F32)
    g = jnp.concatenate([f[i : i + 1] for i in range(16)], axis=1)

    def some(i, _):
        rows = pl.ds(pl.multiple_of(i * 16, 16), 16)
        f = tok[rows, :].astype(F32)
        scaled = f * lax.rsqrt(jnp.mean(f * f, axis=1, keepdims=True) + EPS)
        v = (scaled * g).astype(BF16)
        for y in range(4):
            copied[y, rows, :] = v
        return 0

    lax.fori_loop(0, 8, some, 0, unroll=2)


def cut_body(column, first, ring):
    for z in range(16):
        v = column[z, 0:48, :]
        for x in range(4):
            first[x, z] = v
        ring[z, 0:192, :] = column[z, 48:240, :]
        v = column[z, 240:254, :].astype(F32)
        ring[z, 192:208, :] = jnp.concatenate([v, v[0:2]], axis=0).astype(BF16)


def cum_body(tok, ws, small, spikes, dt, cum, cum_t, edge, square):
    edge[...] = tok[3, 112:128, :]
    n = tok[...].reshape(ROWS, 2048)
    square[...] = jnp.zeros(square.shape, F32)
    square[0, 0:2, :] = small[17:19, 0:128]
    columns = square[0].T[0:4, :]
    raw = dot_nt(ws[...], n) + columns[:, 0:1]
    step = jnp.maximum(raw, 0.0) + jnp.log1p(jnp.exp(-jnp.abs(raw)))
    logs = -step * jnp.exp(columns[:, 1:2]) + spikes[...]
    square[0] = jnp.zeros((BLK, BLK), F32)
    r = lax.broadcasted_iota(jnp.int32, (BLK, BLK), 0)
    s = lax.broadcasted_iota(jnp.int32, (BLK, BLK), 1)
    upper = jnp.where(r <= s, 1.0, 0.0).astype(F32)
    carry = jnp.zeros((4, 1), F32)
    for b in range(NB):
        rows = slice(b * BLK, (b + 1) * BLK)
        part = (
            jnp.dot(
                logs[:, rows],
                upper,
                precision=lax.Precision.HIGHEST,
                preferred_element_type=F32,
            )
            + carry
        )
        cum_t[0:4, rows] = part
        square[0, 0:4, :] = part
        square[1, 0:4, :] = step[:, rows]
        cum[rows, :] = square[0].T
        dt[rows, :] = square[1].T
        carry = part[:, BLK - 1 : BLK]


def fetches(tok, normed, sem):
    copies = [
        pltpu.make_async_copy(tok.at[y], normed.at[HALO + 128 * y : HALO + 128 * (y + 1)], sem.at[y])
        for y in range(4)
    ]
    for copy in copies:
        copy.start()
    return copies


def first_body(
    tok, halo, own, other, dt, cum, small,
    weighted, seq_input, seq_write, local, pieces,
    whole, normed, fields, sem,
):
    fetch = fetches(tok, normed, sem)
    normed[0:HALO, :] = halo[...]
    lay_out(first_pieces(own, other), ((whole, 0, 48),))
    wait_for(fetch)
    projected = dot(normed[...], blocks(whole, 0, 3))
    fields[...] = projected.astype(BF16).astype(F32)
    xin = silu(taps(fields, small[3:7, :], slice(0, 256), 4))
    write = silu(taps(fields, small[7:11, 0:128], slice(256, 384), 4))
    seq_input[...] = xin
    seq_write[...] = write.astype(BF16)
    scaled = xin * per_head(dt[:, 0:128])
    weighted[...] = scaled.astype(BF16)
    state = jnp.zeros((128, 256), F32)
    before = jnp.zeros((1, 128), F32)
    for b in range(NB):
        rows = slice(b * BLK, (b + 1) * BLK)
        end = cum[(b + 1) * BLK - 1 : (b + 1) * BLK, :]
        local[b] = state.astype(BF16)
        to_end = per_head(jnp.exp(end - cum[rows, :]))
        added = dot(write[rows].T.astype(BF16), (scaled[rows] * to_end).astype(BF16))
        state = state * per_head(jnp.exp(end - before)) + added
        before = end
    decay = per_head(jnp.exp(before))
    high = decay.astype(BF16).astype(F32)
    low = decay - high
    tail = jnp.where(
        lax.broadcasted_iota(jnp.int32, (8, 256), 0) < 4,
        jnp.broadcast_to(high, (8, 256)),
        jnp.broadcast_to(low, (8, 256)),
    ).astype(BF16)
    for j in range(8):
        pieces[j, 0:16, :] = state[16 * j : 16 * (j + 1)].astype(BF16)
        pieces[j, 16:24, :] = tail


def piece_of(ref, j):
    v = ref[j].astype(F32)
    return v[0:16], v[16:17] + v[20:21]


def plane_body(got, left, send):
    state = jnp.zeros((16, 256), F32)
    decay = jnp.ones((1, 256), F32)
    for j in range(8):
        s, d = piece_of(got, j)
        state = state * d + s
        decay = decay * d
    high = decay.astype(BF16).astype(F32)
    tail = jnp.where(
        lax.broadcasted_iota(jnp.int32, (8, 256), 0) < 4,
        jnp.broadcast_to(high, (8, 256)),
        jnp.broadcast_to(decay - high, (8, 256)),
    )
    second = lax.broadcasted_iota(jnp.int32, (8, 256), 0) == 1
    tail = jnp.where(second, jnp.broadcast_to(left[...], (8, 256)), tail)
    one = jnp.concatenate([state, tail], axis=0).astype(BF16)
    for k in range(16):
        send[k] = one


def enter_body(got, planes, out):
    z = lax.axis_index("z")
    state = jnp.zeros((16, 256), F32)
    lefts = []
    for k in range(16):
        lefts.append(planes[k].astype(F32)[17:18])
        s, d = piece_of(planes, k)
        state = jnp.where(k < z, state * d + s, state)
    left = jnp.concatenate(lefts, axis=0).astype(BF16)
    for j in range(8):
        out[j, 0:16, :] = state.astype(BF16)
        out[j, 16:32, :] = left
        s, d = piece_of(got, j)
        state = state * d + s


def rest_body(
    tok, halo, p0, p1, p2, p3, p4, p5, p6, p7, small,
    read_out, gate, mixer, wide,
    whole, more, normed, fields, sem, sems,
):
    parts = (p0, p1, p2, p3, p4, p5, p6, p7)
    fetch = fetches(tok, normed, sem)
    one = ring_copies(parts, FAR, whole, 0, 48, sems.at[0])
    two = ring_copies(parts, FAR, more, 48, 96, sems.at[1])
    store = ring_copies(parts, range(8), wide, 144, 64, sems.at[2])
    normed[0:HALO, :] = halo[...]
    lay_out(ring_pieces(parts, NEAR), ((whole, 0, 48), (more, 48, 96)))
    wait_for(fetch)
    wait_for(one)
    n = normed[...]

    def projected(ref, lo, count):
        return dot(n, blocks(ref, lo, count)).astype(BF16).astype(F32)

    fields[:, 0:128] = projected(whole, 0, 1)
    read_out[...] = silu(taps(fields, small[11:15, 0:128], slice(0, 128), 4)).astype(BF16)
    gate[...] = silu(projected(whole, 1, 2)[HALO:])
    wait_for(two)
    inner = projected(more, 2, 2)
    fields[...] = inner * projected(more, 4, 2)
    outer = projected(more, 0, 2)[HALO:]
    mixer[...] = (outer * taps(fields, small[0:3, :], slice(0, 256), 3)).astype(BF16)
    wait_for(store)


def within_body(
    read, weighted, seq_input, seq_write, local, cum, cum_t, small, partly
):
    weight = per_head(small[16:17, 0:128])
    r = lax.broadcasted_iota(jnp.int32, (BLK, BLK), 0)
    s = lax.broadcasted_iota(jnp.int32, (BLK, BLK), 1)
    causal = r >= s
    low = s < 64
    before = jnp.zeros((1, 128), F32)
    for b in range(NB):
        rows = slice(b * BLK, (b + 1) * BLK)
        rb = read[rows, :]
        scores = dot_nt(rb, seq_write[rows, :])
        here = cum[rows, :]
        from_local = dot(rb, local[b]) * per_head(jnp.exp(here - before))
        before = here[BLK - 1 : BLK, :]
        halves = []
        for p in range(2):
            pair = weighted[rows, 128 * p : 128 * (p + 1)]
            two = []
            for h in (2 * p, 2 * p + 1):
                gap = here[:, h : h + 1] - cum_t[h : h + 1, rows]
                damped = scores * jnp.exp(jnp.where(causal, gap, -jnp.inf))
                two.append(dot(damped.astype(BF16), pair))
            halves.append(jnp.where(low, two[0], two[1]))
        within = jnp.concatenate(halves, axis=1)
        partly[rows, :] = within + from_local + weight * seq_input[rows, :]


def patch(wide, arriving):
    row = lax.broadcasted_iota(jnp.int32, (16, 128), 0)
    for j in range(8):
        lefts = arriving[j, 16:32, :].astype(F32)
        for z in range(16):
            tile = wide[z, j // 2, j % 2, 48:64, :].astype(F32)
            for i in range(2):
                v = lefts[z : z + 1, 128 * i : 128 * (i + 1)]
                tile = jnp.where(row == 14 + i, jnp.broadcast_to(v, (16, 128)), tile)
            wide[z, j // 2, j % 2, 48:64, :] = tile.astype(BF16)


def project_out(act, at, wide, out):
    a = act[pl.ds(pl.multiple_of(at * 128, 128), 128), :]
    for q in range(4):
        zs = slice(4 * q, 4 * (q + 1))
        w = [wide[zs, :, :, 16 * k : 16 * (k + 1), :].reshape(512, 128) for k in range(4)]
        w = jnp.concatenate(w, axis=1)
        out[:, 512 * q : 512 * (q + 1)] = dot_nt(a, w).astype(out.dtype)


def tail_body(
    arriving, partly, read, gate, cum, mixer, small, stored, act, far, wide, sem
):
    fetch = pltpu.make_async_copy(stored, wide, sem)
    fetch.start()
    act[:, 0:256] = mixer[...]
    state = jnp.concatenate([arriving[j, 0:16, :] for j in range(8)], axis=0)
    head = partly[...] + dot(read[...], state) * per_head(jnp.exp(cum[...]))
    gated = head * gate[...]
    square = gated * gated
    r = lax.broadcasted_iota(jnp.int32, (256, 256), 0) // 64
    s = lax.broadcasted_iota(jnp.int32, (256, 256), 1) // 64
    same = jnp.where(r == s, 1.0 / 64.0, 0.0).astype(BF16)
    high = square.astype(BF16)
    rest = (square - high.astype(F32)).astype(BF16)
    mean = dot(high, same) + dot(rest, same)
    act[:, 256:512] = (gated * lax.rsqrt(mean + EPS) * small[15:16, :]).astype(BF16)
    fetch.wait()
    patch(wide, arriving)
    project_out(act, (lax.axis_index("tp") + 2) % 4, wide, far)


def near_body(act, wide, beside, near, mine):
    y, c = lax.axis_index("tp"), lax.axis_index("c")
    project_out(act, (y + 3 + 2 * c) % 4, wide, beside)
    project_out(act, (y + 1 + 2 * c) % 4, wide, near)
    project_out(act, y, wide, mine)


def add_body(near, got, out):
    out[...] = (near[...].astype(F32) + got[...].astype(F32)).astype(BF16)


def sum_body(mine, a, b, out):
    v = mine[...].astype(F32) + a[...].astype(F32)
    out[...] = (v + b[...].astype(F32)).astype(BF16)


def exchanged(tiles, axis):
    return lax.all_to_all(tiles, axis, 0, 0, tiled=True)


def two_way(shard, axis, toward):
    steps = [(i, c, (i + (toward if c == 0 else -toward)) % 4) for i in range(4) for c in range(2)]
    if axis == "x":
        return lax.ppermute(shard, ("x", "c"), [(2 * i + c, 2 * j + c) for i, c, j in steps])
    return lax.ppermute(shard, ("c", "tp"), [(4 * c + i, 4 * c + j) for i, c, j in steps])


def swapped(shard):
    return lax.ppermute(shard, "c", [(0, 1), (1, 0)])


def per_device(
    tokens,
    input_norm_scale,
    outer_gate_weight,
    inner_gate_weight,
    value_weight_matrix,
    output_gate_weight,
    state_input_weight,
    write_key_weight,
    read_key_weight,
    step_size_weight,
    gated_conv_weight,
    input_conv_weight,
    write_conv_weight,
    read_conv_weight,
    step_size_bias,
    log_decay_rate,
    decay_spikes,
    direct_path_weight,
    head_norm_scale,
    conv_output_weight,
    state_output_weight,
):
    copied, own, left, small = call(
        prep_body,
        (
            shape((4, 128, 2048), BF16),
            shape((254, 128), BF16),
            shape((1, 256), F32),
            shape((24, 256), F32),
        ),
        (
            tokens,
            input_norm_scale.reshape(16, 128),
            state_input_weight,
            write_key_weight,
            read_key_weight,
            output_gate_weight,
            outer_gate_weight,
            inner_gate_weight,
            value_weight_matrix,
            conv_output_weight.T,
            state_output_weight.T,
            gated_conv_weight,
            input_conv_weight,
            write_conv_weight,
            read_conv_weight,
            head_norm_scale.reshape(2, 128),
            direct_path_weight[None],
            step_size_bias[None],
            log_decay_rate[None],
        ),
        mib=None,
    )
    tok = exchanged(copied, "tp")
    column = lax.all_gather(own, "z", axis=0, tiled=False)
    first, ring = call(
        cut_body,
        (main_memory((4, 16, 48, 128), BF16), main_memory((16, 208, 128), BF16)),
        (column,),
    )
    first = exchanged(first, "x")
    first_other = swapped(first)
    ring = [ring]
    ring.append(two_way(ring[0], "x", 1))
    ring.append(two_way(ring[0], "x", -1))
    ring.append(two_way(ring[1], "x", 1))
    ring += [swapped(part) for part in ring]
    dt, cum, cum_t, edge = call(
        cum_body,
        (
            shape((ROWS, 128), F32),
            shape((ROWS, 128), F32),
            shape((8, ROWS), F32),
            shape((HALO, 2048), BF16),
        ),
        (tok, step_size_weight.T, small, decay_spikes),
        scratch=(pltpu.VMEM((2, BLK, BLK), F32),),
    )
    halo = lax.ppermute(edge, SP, [(i, i + 1) for i in range(127)])
    weighted, seq_input, seq_write, local, pieces = call(
        first_body,
        (
            main_memory((ROWS, 256), BF16),
            main_memory((ROWS, 256), F32),
            main_memory((ROWS, 128), BF16),
            main_memory((NB, 128, 256), BF16),
            main_memory((8, 24, 256), BF16),
        ),
        (tok, halo, first, first_other, dt, cum, small),
        (
            pltpu.VMEM((16, 4, 2, 48, 128), BF16),
            pltpu.VMEM((HALO + ROWS, 2048), BF16),
            pltpu.VMEM((HALO + ROWS, 384), F32),
            pltpu.SemaphoreType.DMA((4,)),
        ),
        mib=16,
        far_in=(0,),
    )
    got = exchanged(pieces, ("x", "c"))
    send = call(plane_body, shape((16, 24, 256), BF16), (got, left))
    planes = exchanged(send, "z")
    entering = call(enter_body, shape((8, 32, 256), BF16), (got, planes))
    arriving = exchanged(entering, ("x", "c"))

    read, gate, mixer, wide = call(
        rest_body,
        (
            on_chip((ROWS, 128), BF16),
            on_chip((ROWS, 256), F32),
            on_chip((ROWS, 256), BF16),
            main_memory((16, 4, 2, 64, 128), BF16),
        ),
        (tok, halo, *ring, small),
        scratch=(
            pltpu.VMEM((16, 4, 2, 48, 128), BF16),
            pltpu.VMEM((16, 4, 2, 96, 128), BF16),
            pltpu.VMEM((HALO + ROWS, 2048), BF16),
            pltpu.VMEM((HALO + ROWS, 256), F32),
            pltpu.SemaphoreType.DMA((4,)),
            pltpu.SemaphoreType.DMA((3, 8)),
        ),
        mib=20,
        far_in=(0, *(2 + i for i in FAR)),
        far_out=(3,),
    )
    partly = call(
        within_body,
        shape((ROWS, 256), F32),
        (read, weighted, seq_input, seq_write, local, cum, cum_t, small),
    )
    act, far, wide = call(
        tail_body,
        (
            on_chip((ROWS, 512), BF16),
            shape((128, 2048), BF16),
            on_chip((16, 4, 2, 64, 128), BF16),
        ),
        (arriving, partly, read, gate, cum, mixer, small, wide),
        scratch=(pltpu.SemaphoreType.DMA,),
        mib=16,
        far_in=(7,),
    )
    got_far = two_way(far, "tp", 1)
    block_ = shape((128, 2048), BF16)
    beside, near, mine = call(near_body, (block_, block_, block_), (act, wide), mib=12)
    got_beside = two_way(beside, "tp", -1)
    both = call(add_body, shape((128, 2048), BF16), (near, got_far))
    got_near = two_way(both, "tp", 1)
    return call(sum_body, shape((128, 2048), BF16), (mine, got_beside, got_near))


def solution(mesh):
    torus = Mesh(mesh.devices.reshape(16, 4, 2, mesh.shape["tp"]), SP_TP)
    rows = P(SP, "tp")
    cols = P("tp", SP)
    taps_ = P(None, "tp")
    heads = P("tp")
    return jax.shard_map(
        per_device,
        mesh=torus,
        in_specs=(
            P(SP_TP, None), P(), rows, rows, rows, rows, rows, rows, rows,
            taps_, taps_, taps_, taps_, taps_, heads, heads, cols, heads, heads, cols, cols,
        ),
        out_specs=P(SP_TP, None),
        check_vma=False,
    )
```

```python
import jax
import jax.numpy as jnp
from jax import lax
from jax.experimental import pallas as pl
from jax.experimental.pallas import tpu as pltpu
from jax.sharding import Mesh
from jax.sharding import PartitionSpec as P

SP = ("z", "x", "c")
SP_TP = ("z", "x", "c", "tp")
EPS = 1e-05
ROWS = 512
HALO = 16
BLK = 128
NB = ROWS // BLK
F32 = jnp.float32
BF16 = jnp.bfloat16


def call(body, outs, args, scratch=(), mib=8, far_in=(), far_out=()):
    vmem = pl.BlockSpec(memory_space=pltpu.VMEM)
    hbm = pl.BlockSpec(memory_space=pltpu.HBM)
    many = isinstance(outs, tuple)
    args = [
        pltpu.with_memory_space_constraint(a, pltpu.HBM) if i in far_in else a
        for i, a in enumerate(args)
    ]
    return pl.pallas_call(
        body,
        out_shape=outs,
        in_specs=[hbm if i in far_in else vmem for i in range(len(args))],
        out_specs=tuple(hbm if i in far_out else vmem for i in range(len(outs))) if many else vmem,
        scratch_shapes=list(scratch),
        compiler_params=pltpu.CompilerParams(
            vmem_limit_bytes=None if mib is None else mib * 2**20
        ),
    )(*args)


def shape(dims, kind):
    return jax.ShapeDtypeStruct(dims, kind)


def on_chip(dims, kind):
    return pltpu.VMEM(dims, kind)


def main_memory(dims, kind):
    return pltpu.HBM(dims, kind)


def dot(a, b):
    return jnp.dot(a, b, preferred_element_type=F32)


def dot_nt(a, b):
    return lax.dot_general(a, b, (((1,), (1,)), ((), ())), preferred_element_type=F32)


def per_head(v):
    rows = v.shape[0]
    low = lax.broadcasted_iota(jnp.int32, (rows, 128), 1) < 64
    pairs = [
        jnp.where(
            low,
            jnp.broadcast_to(v[:, 2 * p : 2 * p + 1], (rows, 128)),
            jnp.broadcast_to(v[:, 2 * p + 1 : 2 * p + 2], (rows, 128)),
        )
        for p in range(2)
    ]
    return jnp.concatenate(pairs, axis=1)


def silu(v):
    return v / (1.0 + jnp.exp(-v))


def lay_out(pieces, targets):
    def some(z, _):
        for get, x, c in pieces:
            for ref, lo, count in targets:
                ref[z, x, c] = get(z, lo, count)
        return 0

    lax.fori_loop(0, 16, some, 0)


def first_pieces(own, other):
    c = lax.axis_index("c")
    return [
        (lambda z, lo, n, r=ref, x=x: r[x, z, lo : lo + n, :], x, at)
        for ref, at in ((own, c), (other, 1 - c))
        for x in range(4)
    ]


def ring_places():
    x, c = lax.axis_index("x"), lax.axis_index("c")
    return [
        ((x + by) % 4, at)
        for at in (c, 1 - c)
        for by in (0, 3 - 2 * at, 1 + 2 * at, 2)
    ]


def ring_copies(parts, which, target, lo, count, sems):
    places = ring_places()
    copies = []
    for i in which:
        x, at = places[i]
        copies.append(
            pltpu.make_async_copy(
                parts[i].at[:, lo : lo + count, :], target.at[:, x, at], sems.at[i]
            )
        )
    for copy in copies:
        copy.start()
    return copies


def ring_pieces(parts, which):
    places = ring_places()
    return [
        (lambda z, lo, n, r=parts[i]: r[z, lo : lo + n, :], *places[i]) for i in which
    ]


FAR = (0, 1, 2, 4)
NEAR = (3, 5, 6, 7)


def wait_for(copies):
    for copy in copies:
        copy.wait()


def block(whole, q):
    return whole[:, :, :, 16 * q : 16 * (q + 1), :].reshape(2048, 128)


def blocks(whole, lo, count):
    return jnp.concatenate([block(whole, q) for q in range(lo, lo + count)], axis=1)


def taps(ref, w, cols, count):
    out = None
    for k in range(count):
        part = w[k : k + 1, :] * ref[pl.ds(HALO - count + 1 + k, ROWS), cols]
        out = part if out is None else out + part
    return out


def prep_body(
    tok, gain, w0, w1, w2, w3, w4, w5, w6, w7, w8,
    gated_taps, input_taps, write_taps, read_taps, scale, direct, bias, rate,
    copied, own, left, small,
):
    q = 0
    for w in (w0, w1, w2, w3, w4, w5, w6, w7, w8):
        for k in range(w.shape[1] // 128):
            v = w[:, 128 * k : 128 * (k + 1)]
            if q < 15:
                own[16 * q : 16 * (q + 1), :] = v
            else:
                own[240:254, :] = v[0:14]
                f = v.astype(F32)
                left[...] = jnp.concatenate([f[14:15], f[15:16]], axis=1)
            q += 1
    small[...] = jnp.zeros(small.shape, F32)
    small[0:3, :] = gated_taps[...].astype(F32)
    small[3:7, :] = input_taps[...].astype(F32)
    small[7:11, 0:128] = write_taps[...].astype(F32)
    small[11:15, 0:128] = read_taps[...].astype(F32)
    f = scale[...].astype(F32)
    small[15:16, :] = jnp.concatenate([f[0:1], f[1:2]], axis=1)
    small[16:17, 0:4] = direct[...]
    small[17:18, 0:4] = bias[...]
    small[18:19, 0:4] = rate[...]
    f = gain[...].astype(F32)
    g = jnp.concatenate([f[i : i + 1] for i in range(16)], axis=1)

    def some(i, _):
        rows = pl.ds(pl.multiple_of(i * 16, 16), 16)
        f = tok[rows, :].astype(F32)
        scaled = f * lax.rsqrt(jnp.mean(f * f, axis=1, keepdims=True) + EPS)
        v = (scaled * g).astype(BF16)
        for y in range(4):
            copied[y, rows, :] = v
        return 0

    lax.fori_loop(0, 8, some, 0, unroll=2)


def cut_body(column, first, ring):
    for z in range(16):
        v = column[z, 0:48, :]
        for x in range(4):
            first[x, z] = v
        ring[z, 0:192, :] = column[z, 48:240, :]
        v = column[z, 240:254, :].astype(F32)
        ring[z, 192:208, :] = jnp.concatenate([v, v[0:2]], axis=0).astype(BF16)


def cum_body(tok, ws, small, spikes, dt, cum, cum_t, edge, square):
    edge[...] = tok[3, 112:128, :]
    n = tok[...].reshape(ROWS, 2048)
    square[...] = jnp.zeros(square.shape, F32)
    square[0, 0:2, :] = small[17:19, 0:128]
    columns = square[0].T[0:4, :]
    raw = dot_nt(ws[...], n) + columns[:, 0:1]
    step = jnp.maximum(raw, 0.0) + jnp.log1p(jnp.exp(-jnp.abs(raw)))
    logs = -step * jnp.exp(columns[:, 1:2]) + spikes[...]
    square[0] = jnp.zeros((BLK, BLK), F32)
    r = lax.broadcasted_iota(jnp.int32, (BLK, BLK), 0)
    s = lax.broadcasted_iota(jnp.int32, (BLK, BLK), 1)
    upper = jnp.where(r <= s, 1.0, 0.0).astype(F32)
    carry = jnp.zeros((4, 1), F32)
    for b in range(NB):
        rows = slice(b * BLK, (b + 1) * BLK)
        part = (
            jnp.dot(
                logs[:, rows],
                upper,
                precision=lax.Precision.HIGHEST,
                preferred_element_type=F32,
            )
            + carry
        )
        cum_t[0:4, rows] = part
        square[0, 0:4, :] = part
        square[1, 0:4, :] = step[:, rows]
        cum[rows, :] = square[0].T
        dt[rows, :] = square[1].T
        carry = part[:, BLK - 1 : BLK]


def fetches(tok, normed, sem):
    copies = [
        pltpu.make_async_copy(tok.at[y], normed.at[HALO + 128 * y : HALO + 128 * (y + 1)], sem.at[y])
        for y in range(4)
    ]
    for copy in copies:
        copy.start()
    return copies


def first_body(
    tok, halo, own, other, dt, cum, small,
    weighted, seq_input, seq_write, local, pieces,
    whole, normed, fields, sem,
):
    fetch = fetches(tok, normed, sem)
    normed[0:HALO, :] = halo[...]
    lay_out(first_pieces(own, other), ((whole, 0, 48),))
    wait_for(fetch)
    projected = dot(normed[...], blocks(whole, 0, 3))
    fields[...] = projected.astype(BF16).astype(F32)
    xin = silu(taps(fields, small[3:7, :], slice(0, 256), 4))
    write = silu(taps(fields, small[7:11, 0:128], slice(256, 384), 4))
    seq_input[...] = xin
    seq_write[...] = write.astype(BF16)
    scaled = xin * per_head(dt[:, 0:128])
    weighted[...] = scaled.astype(BF16)
    state = jnp.zeros((128, 256), F32)
    before = jnp.zeros((1, 128), F32)
    for b in range(NB):
        rows = slice(b * BLK, (b + 1) * BLK)
        end = cum[(b + 1) * BLK - 1 : (b + 1) * BLK, :]
        local[b] = state.astype(BF16)
        to_end = per_head(jnp.exp(end - cum[rows, :]))
        added = dot(write[rows].T.astype(BF16), (scaled[rows] * to_end).astype(BF16))
        state = state * per_head(jnp.exp(end - before)) + added
        before = end
    decay = per_head(jnp.exp(before))
    high = decay.astype(BF16).astype(F32)
    low = decay - high
    tail = jnp.where(
        lax.broadcasted_iota(jnp.int32, (8, 256), 0) < 4,
        jnp.broadcast_to(high, (8, 256)),
        jnp.broadcast_to(low, (8, 256)),
    ).astype(BF16)
    for j in range(8):
        pieces[j, 0:16, :] = state[16 * j : 16 * (j + 1)].astype(BF16)
        pieces[j, 16:24, :] = tail


def piece_of(ref, j):
    v = ref[j].astype(F32)
    return v[0:16], v[16:17] + v[20:21]


def plane_body(got, left, send):
    state = jnp.zeros((16, 256), F32)
    decay = jnp.ones((1, 256), F32)
    for j in range(8):
        s, d = piece_of(got, j)
        state = state * d + s
        decay = decay * d
    high = decay.astype(BF16).astype(F32)
    tail = jnp.where(
        lax.broadcasted_iota(jnp.int32, (8, 256), 0) < 4,
        jnp.broadcast_to(high, (8, 256)),
        jnp.broadcast_to(decay - high, (8, 256)),
    )
    second = lax.broadcasted_iota(jnp.int32, (8, 256), 0) == 1
    tail = jnp.where(second, jnp.broadcast_to(left[...], (8, 256)), tail)
    one = jnp.concatenate([state, tail], axis=0).astype(BF16)
    for k in range(16):
        send[k] = one


def enter_body(got, planes, out):
    z = lax.axis_index("z")
    state = jnp.zeros((16, 256), F32)
    lefts = []
    for k in range(16):
        lefts.append(planes[k].astype(F32)[17:18])
        s, d = piece_of(planes, k)
        state = jnp.where(k < z, state * d + s, state)
    left = jnp.concatenate(lefts, axis=0).astype(BF16)
    for j in range(8):
        out[j, 0:16, :] = state.astype(BF16)
        out[j, 16:32, :] = left
        s, d = piece_of(got, j)
        state = state * d + s


def rest_body(
    tok, halo, p0, p1, p2, p3, p4, p5, p6, p7, small,
    read_out, gate, mixer, wide,
    whole, more, laid, normed, fields, sem, sems, store_sem,
):
    parts = (p0, p1, p2, p3, p4, p5, p6, p7)
    fetch = fetches(tok, normed, sem)
    one = ring_copies(parts, FAR, whole, 0, 48, sems.at[0])
    two = ring_copies(parts, FAR, more, 48, 96, sems.at[1])
    three = ring_copies(parts, FAR, laid, 144, 64, sems.at[2])
    normed[0:HALO, :] = halo[...]
    lay_out(ring_pieces(parts, NEAR), ((whole, 0, 48), (more, 48, 96), (laid, 144, 64)))
    wait_for(fetch)
    wait_for(one)
    n = normed[...]

    def projected(ref, lo, count):
        return dot(n, blocks(ref, lo, count)).astype(BF16).astype(F32)

    fields[:, 0:128] = projected(whole, 0, 1)
    read_out[...] = silu(taps(fields, small[11:15, 0:128], slice(0, 128), 4)).astype(BF16)
    gate[...] = silu(projected(whole, 1, 2)[HALO:])
    wait_for(three)
    store = pltpu.make_async_copy(laid, wide, store_sem)
    store.start()
    wait_for(two)
    inner = projected(more, 2, 2)
    fields[...] = inner * projected(more, 4, 2)
    outer = projected(more, 0, 2)[HALO:]
    mixer[...] = (outer * taps(fields, small[0:3, :], slice(0, 256), 3)).astype(BF16)
    store.wait()


def within_body(
    read, weighted, seq_input, seq_write, local, cum, cum_t, small, partly
):
    weight = per_head(small[16:17, 0:128])
    r = lax.broadcasted_iota(jnp.int32, (BLK, BLK), 0)
    s = lax.broadcasted_iota(jnp.int32, (BLK, BLK), 1)
    causal = r >= s
    low = s < 64
    before = jnp.zeros((1, 128), F32)
    for b in range(NB):
        rows = slice(b * BLK, (b + 1) * BLK)
        rb = read[rows, :]
        scores = dot_nt(rb, seq_write[rows, :])
        here = cum[rows, :]
        from_local = dot(rb, local[b]) * per_head(jnp.exp(here - before))
        before = here[BLK - 1 : BLK, :]
        halves = []
        for p in range(2):
            pair = weighted[rows, 128 * p : 128 * (p + 1)]
            two = []
            for h in (2 * p, 2 * p + 1):
                gap = here[:, h : h + 1] - cum_t[h : h + 1, rows]
                damped = scores * jnp.exp(jnp.where(causal, gap, -jnp.inf))
                two.append(dot(damped.astype(BF16), pair))
            halves.append(jnp.where(low, two[0], two[1]))
        within = jnp.concatenate(halves, axis=1)
        partly[rows, :] = within + from_local + weight * seq_input[rows, :]


def patch(wide, arriving):
    row = lax.broadcasted_iota(jnp.int32, (16, 128), 0)
    for j in range(8):
        lefts = arriving[j, 16:32, :].astype(F32)
        for z in range(16):
            tile = wide[z, j // 2, j % 2, 48:64, :].astype(F32)
            for i in range(2):
                v = lefts[z : z + 1, 128 * i : 128 * (i + 1)]
                tile = jnp.where(row == 14 + i, jnp.broadcast_to(v, (16, 128)), tile)
            wide[z, j // 2, j % 2, 48:64, :] = tile.astype(BF16)


def project_out(act, at, wide, out):
    a = act[pl.ds(pl.multiple_of(at * 128, 128), 128), :]
    for q in range(4):
        zs = slice(4 * q, 4 * (q + 1))
        w = [wide[zs, :, :, 16 * k : 16 * (k + 1), :].reshape(512, 128) for k in range(4)]
        w = jnp.concatenate(w, axis=1)
        out[:, 512 * q : 512 * (q + 1)] = dot_nt(a, w).astype(out.dtype)


def tail_body(
    arriving, partly, read, gate, cum, mixer, small, stored, act, far, wide, sem
):
    fetch = pltpu.make_async_copy(stored, wide, sem)
    fetch.start()
    act[:, 0:256] = mixer[...]
    state = jnp.concatenate([arriving[j, 0:16, :] for j in range(8)], axis=0)
    head = partly[...] + dot(read[...], state) * per_head(jnp.exp(cum[...]))
    gated = head * gate[...]
    square = gated * gated
    r = lax.broadcasted_iota(jnp.int32, (256, 256), 0) // 64
    s = lax.broadcasted_iota(jnp.int32, (256, 256), 1) // 64
    same = jnp.where(r == s, 1.0 / 64.0, 0.0).astype(BF16)
    high = square.astype(BF16)
    rest = (square - high.astype(F32)).astype(BF16)
    mean = dot(high, same) + dot(rest, same)
    act[:, 256:512] = (gated * lax.rsqrt(mean + EPS) * small[15:16, :]).astype(BF16)
    fetch.wait()
    patch(wide, arriving)
    project_out(act, (lax.axis_index("tp") + 2) % 4, wide, far)


def near_body(act, wide, beside, near, mine):
    y, c = lax.axis_index("tp"), lax.axis_index("c")
    project_out(act, (y + 3 + 2 * c) % 4, wide, beside)
    project_out(act, (y + 1 + 2 * c) % 4, wide, near)
    project_out(act, y, wide, mine)


def add_body(near, got, out):
    out[...] = (near[...].astype(F32) + got[...].astype(F32)).astype(BF16)


def sum_body(mine, a, b, out):
    v = mine[...].astype(F32) + a[...].astype(F32)
    out[...] = (v + b[...].astype(F32)).astype(BF16)


def exchanged(tiles, axis):
    return lax.all_to_all(tiles, axis, 0, 0, tiled=True)


def two_way(shard, axis, toward):
    steps = [(i, c, (i + (toward if c == 0 else -toward)) % 4) for i in range(4) for c in range(2)]
    if axis == "x":
        return lax.ppermute(shard, ("x", "c"), [(2 * i + c, 2 * j + c) for i, c, j in steps])
    return lax.ppermute(shard, ("c", "tp"), [(4 * c + i, 4 * c + j) for i, c, j in steps])


def swapped(shard):
    return lax.ppermute(shard, "c", [(0, 1), (1, 0)])


def per_device(
    tokens,
    input_norm_scale,
    outer_gate_weight,
    inner_gate_weight,
    value_weight_matrix,
    output_gate_weight,
    state_input_weight,
    write_key_weight,
    read_key_weight,
    step_size_weight,
    gated_conv_weight,
    input_conv_weight,
    write_conv_weight,
    read_conv_weight,
    step_size_bias,
    log_decay_rate,
    decay_spikes,
    direct_path_weight,
    head_norm_scale,
    conv_output_weight,
    state_output_weight,
):
    copied, own, left, small = call(
        prep_body,
        (
            shape((4, 128, 2048), BF16),
            shape((254, 128), BF16),
            shape((1, 256), F32),
            shape((24, 256), F32),
        ),
        (
            tokens,
            input_norm_scale.reshape(16, 128),
            state_input_weight,
            write_key_weight,
            read_key_weight,
            output_gate_weight,
            outer_gate_weight,
            inner_gate_weight,
            value_weight_matrix,
            conv_output_weight.T,
            state_output_weight.T,
            gated_conv_weight,
            input_conv_weight,
            write_conv_weight,
            read_conv_weight,
            head_norm_scale.reshape(2, 128),
            direct_path_weight[None],
            step_size_bias[None],
            log_decay_rate[None],
        ),
        mib=None,
    )
    tok = exchanged(copied, "tp")
    column = lax.all_gather(own, "z", axis=0, tiled=False)
    first, ring = call(
        cut_body,
        (main_memory((4, 16, 48, 128), BF16), main_memory((16, 208, 128), BF16)),
        (column,),
    )
    first = exchanged(first, "x")
    first_other = swapped(first)
    ring = [ring]
    ring.append(two_way(ring[0], "x", 1))
    ring.append(two_way(ring[0], "x", -1))
    ring.append(two_way(ring[1], "x", 1))
    ring += [swapped(part) for part in ring]
    dt, cum, cum_t, edge = call(
        cum_body,
        (
            shape((ROWS, 128), F32),
            shape((ROWS, 128), F32),
            shape((8, ROWS), F32),
            shape((HALO, 2048), BF16),
        ),
        (tok, step_size_weight.T, small, decay_spikes),
        scratch=(pltpu.VMEM((2, BLK, BLK), F32),),
    )
    halo = lax.ppermute(edge, SP, [(i, i + 1) for i in range(127)])
    weighted, seq_input, seq_write, local, pieces = call(
        first_body,
        (
            main_memory((ROWS, 256), BF16),
            main_memory((ROWS, 256), F32),
            main_memory((ROWS, 128), BF16),
            main_memory((NB, 128, 256), BF16),
            main_memory((8, 24, 256), BF16),
        ),
        (tok, halo, first, first_other, dt, cum, small),
        (
            pltpu.VMEM((16, 4, 2, 48, 128), BF16),
            pltpu.VMEM((HALO + ROWS, 2048), BF16),
            pltpu.VMEM((HALO + ROWS, 384), F32),
            pltpu.SemaphoreType.DMA((4,)),
        ),
        mib=16,
        far_in=(0,),
    )
    got = exchanged(pieces, ("x", "c"))
    send = call(plane_body, shape((16, 24, 256), BF16), (got, left))
    planes = exchanged(send, "z")
    entering = call(enter_body, shape((8, 32, 256), BF16), (got, planes))
    arriving = exchanged(entering, ("x", "c"))

    read, gate, mixer, wide = call(
        rest_body,
        (
            on_chip((ROWS, 128), BF16),
            on_chip((ROWS, 256), F32),
            on_chip((ROWS, 256), BF16),
            main_memory((16, 4, 2, 64, 128), BF16),
        ),
        (tok, halo, *ring, small),
        scratch=(
            pltpu.VMEM((16, 4, 2, 48, 128), BF16),
            pltpu.VMEM((16, 4, 2, 96, 128), BF16),
            pltpu.VMEM((16, 4, 2, 64, 128), BF16),
            pltpu.VMEM((HALO + ROWS, 2048), BF16),
            pltpu.VMEM((HALO + ROWS, 256), F32),
            pltpu.SemaphoreType.DMA((4,)),
            pltpu.SemaphoreType.DMA((3, 8)),
            pltpu.SemaphoreType.DMA,
        ),
        mib=24,
        far_in=(0, *(2 + i for i in FAR)),
        far_out=(3,),
    )
    partly = call(
        within_body,
        shape((ROWS, 256), F32),
        (read, weighted, seq_input, seq_write, local, cum, cum_t, small),
    )
    act, far, wide = call(
        tail_body,
        (
            on_chip((ROWS, 512), BF16),
            shape((128, 2048), BF16),
            on_chip((16, 4, 2, 64, 128), BF16),
        ),
        (arriving, partly, read, gate, cum, mixer, small, wide),
        scratch=(pltpu.SemaphoreType.DMA,),
        mib=16,
        far_in=(7,),
    )
    got_far = two_way(far, "tp", 1)
    block_ = shape((128, 2048), BF16)
    beside, near, mine = call(near_body, (block_, block_, block_), (act, wide), mib=12)
    got_beside = two_way(beside, "tp", -1)
    both = call(add_body, shape((128, 2048), BF16), (near, got_far))
    got_near = two_way(both, "tp", 1)
    return call(sum_body, shape((128, 2048), BF16), (mine, got_beside, got_near))


def solution(mesh):
    torus = Mesh(mesh.devices.reshape(16, 4, 2, mesh.shape["tp"]), SP_TP)
    rows = P(SP, "tp")
    cols = P("tp", SP)
    taps_ = P(None, "tp")
    heads = P("tp")
    return jax.shard_map(
        per_device,
        mesh=torus,
        in_specs=(
            P(SP_TP, None), P(), rows, rows, rows, rows, rows, rows, rows,
            taps_, taps_, taps_, taps_, taps_, heads, heads, cols, heads, heads, cols, cols,
        ),
        out_specs=P(SP_TP, None),
        check_vma=False,
    )
```

```python
import jax
import jax.numpy as jnp
from jax import lax
from jax.experimental import pallas as pl
from jax.experimental.pallas import tpu as pltpu
from jax.sharding import Mesh
from jax.sharding import PartitionSpec as P

SP = ("z", "x", "c")
SP_TP = ("z", "x", "c", "tp")
EPS = 1e-05
ROWS = 512
HALO = 16
BLK = 128
NB = ROWS // BLK
F32 = jnp.float32
BF16 = jnp.bfloat16


def call(body, outs, args, scratch=(), mib=8, far_in=(), far_out=()):
    vmem = pl.BlockSpec(memory_space=pltpu.VMEM)
    hbm = pl.BlockSpec(memory_space=pltpu.HBM)
    many = isinstance(outs, tuple)
    args = [
        pltpu.with_memory_space_constraint(a, pltpu.HBM) if i in far_in else a
        for i, a in enumerate(args)
    ]
    return pl.pallas_call(
        body,
        out_shape=outs,
        in_specs=[hbm if i in far_in else vmem for i in range(len(args))],
        out_specs=tuple(hbm if i in far_out else vmem for i in range(len(outs))) if many else vmem,
        scratch_shapes=list(scratch),
        compiler_params=pltpu.CompilerParams(
            vmem_limit_bytes=None if mib is None else mib * 2**20
        ),
    )(*args)


def shape(dims, kind):
    return jax.ShapeDtypeStruct(dims, kind)


def on_chip(dims, kind):
    return pltpu.VMEM(dims, kind)


def main_memory(dims, kind):
    return pltpu.HBM(dims, kind)


def dot(a, b):
    return jnp.dot(a, b, preferred_element_type=F32)


def dot_nt(a, b):
    return lax.dot_general(a, b, (((1,), (1,)), ((), ())), preferred_element_type=F32)


def per_head(v):
    rows = v.shape[0]
    low = lax.broadcasted_iota(jnp.int32, (rows, 128), 1) < 64
    pairs = [
        jnp.where(
            low,
            jnp.broadcast_to(v[:, 2 * p : 2 * p + 1], (rows, 128)),
            jnp.broadcast_to(v[:, 2 * p + 1 : 2 * p + 2], (rows, 128)),
        )
        for p in range(2)
    ]
    return jnp.concatenate(pairs, axis=1)


def silu(v):
    return v / (1.0 + jnp.exp(-v))


def lay_out(pieces, targets):
    def some(z, _):
        for get, x, c in pieces:
            for ref, lo, count in targets:
                ref[z, x, c] = get(z, lo, count)
        return 0

    lax.fori_loop(0, 16, some, 0)


def first_pieces(own, other):
    c = lax.axis_index("c")
    return [
        (lambda z, lo, n, r=ref, x=x: r[x, z, lo : lo + n, :], x, at)
        for ref, at in ((own, c), (other, 1 - c))
        for x in range(4)
    ]


def ring_places():
    x, c = lax.axis_index("x"), lax.axis_index("c")
    return [
        ((x + by) % 4, at)
        for at in (c, 1 - c)
        for by in (0, 3 - 2 * at, 1 + 2 * at, 2)
    ]


def ring_copies(parts, which, target, lo, count, sems):
    places = ring_places()
    copies = []
    for i in which:
        x, at = places[i]
        copies.append(
            pltpu.make_async_copy(
                parts[i].at[:, lo : lo + count, :], target.at[:, x, at], sems.at[i]
            )
        )
    for copy in copies:
        copy.start()
    return copies


def ring_pieces(parts, which):
    places = ring_places()
    return [
        (lambda z, lo, n, r=parts[i]: r[z, lo : lo + n, :], *places[i]) for i in which
    ]


FAR = (0, 1, 2, 4)
NEAR = (3, 5, 6, 7)


def wait_for(copies):
    for copy in copies:
        copy.wait()


def block(whole, q):
    return whole[:, :, :, 16 * q : 16 * (q + 1), :].reshape(2048, 128)


def blocks(whole, lo, count):
    return jnp.concatenate([block(whole, q) for q in range(lo, lo + count)], axis=1)


def taps(ref, w, cols, count):
    out = None
    for k in range(count):
        part = w[k : k + 1, :] * ref[pl.ds(HALO - count + 1 + k, ROWS), cols]
        out = part if out is None else out + part
    return out


def prep_body(
    tok, gain, w0, w1, w2, w3, w4, w5, w6, w7, w8,
    gated_taps, input_taps, write_taps, read_taps, scale, direct, bias, rate,
    copied, own, left, small,
):
    q = 0
    for w in (w0, w1, w2, w3, w4, w5, w6, w7, w8):
        for k in range(w.shape[1] // 128):
            v = w[:, 128 * k : 128 * (k + 1)]
            if q < 15:
                own[16 * q : 16 * (q + 1), :] = v
            else:
                own[240:254, :] = v[0:14]
                f = v.astype(F32)
                left[...] = jnp.concatenate([f[14:15], f[15:16]], axis=1)
            q += 1
    small[...] = jnp.zeros(small.shape, F32)
    small[0:3, :] = gated_taps[...].astype(F32)
    small[3:7, :] = input_taps[...].astype(F32)
    small[7:11, 0:128] = write_taps[...].astype(F32)
    small[11:15, 0:128] = read_taps[...].astype(F32)
    f = scale[...].astype(F32)
    small[15:16, :] = jnp.concatenate([f[0:1], f[1:2]], axis=1)
    small[16:17, 0:4] = direct[...]
    small[17:18, 0:4] = bias[...]
    small[18:19, 0:4] = rate[...]
    f = gain[...].astype(F32)
    g = jnp.concatenate([f[i : i + 1] for i in range(16)], axis=1)

    def some(i, _):
        rows = pl.ds(pl.multiple_of(i * 16, 16), 16)
        f = tok[rows, :].astype(F32)
        scaled = f * lax.rsqrt(jnp.mean(f * f, axis=1, keepdims=True) + EPS)
        v = (scaled * g).astype(BF16)
        for y in range(4):
            copied[y, rows, :] = v
        return 0

    lax.fori_loop(0, 8, some, 0, unroll=2)


def cut_body(column, first, ring):
    for z in range(16):
        v = column[z, 0:48, :]
        for x in range(4):
            first[x, z] = v
        ring[z, 0:192, :] = column[z, 48:240, :]
        v = column[z, 240:254, :].astype(F32)
        ring[z, 192:208, :] = jnp.concatenate([v, v[0:2]], axis=0).astype(BF16)


def cum_body(tok, ws, small, spikes, dt_t, cum_t, edge, square):
    edge[...] = tok[3, 112:128, :]
    n = tok[...].reshape(ROWS, 2048)
    square[...] = jnp.zeros(square.shape, F32)
    square[0:2, :] = small[17:19, 0:128]
    columns = square[...].T[0:4, :]
    raw = dot_nt(ws[...], n) + columns[:, 0:1]
    step = jnp.maximum(raw, 0.0) + jnp.log1p(jnp.exp(-jnp.abs(raw)))
    logs = -step * jnp.exp(columns[:, 1:2]) + spikes[...]
    dt_t[...] = jnp.zeros(dt_t.shape, F32)
    cum_t[...] = jnp.zeros(cum_t.shape, F32)
    dt_t[0:4, :] = step
    r = lax.broadcasted_iota(jnp.int32, (BLK, BLK), 0)
    s = lax.broadcasted_iota(jnp.int32, (BLK, BLK), 1)
    upper = jnp.where(r <= s, 1.0, 0.0).astype(F32)
    carry = jnp.zeros((4, 1), F32)
    for b in range(NB):
        rows = slice(b * BLK, (b + 1) * BLK)
        part = (
            jnp.dot(
                logs[:, rows],
                upper,
                precision=lax.Precision.HIGHEST,
                preferred_element_type=F32,
            )
            + carry
        )
        cum_t[0:4, rows] = part
        carry = part[:, BLK - 1 : BLK]


def by_position(ref, start):
    part = ref[:, start : start + BLK]
    return jnp.concatenate([part, jnp.zeros((BLK - 8, BLK), F32)], axis=0).T


def fetches(tok, normed, sem):
    copies = [
        pltpu.make_async_copy(tok.at[y], normed.at[HALO + 128 * y : HALO + 128 * (y + 1)], sem.at[y])
        for y in range(4)
    ]
    for copy in copies:
        copy.start()
    return copies


def first_body(
    tok, halo, own, other, dt_t, cum_t, small,
    weighted, seq_input, seq_write, local, pieces,
    whole, normed, fields,
):
    normed[0:HALO, :] = halo[...]
    normed[HALO:, :] = tok[...].reshape(ROWS, 2048)
    lay_out(first_pieces(own, other), ((whole, 0, 48),))
    projected = dot(normed[...], blocks(whole, 0, 3))
    fields[...] = projected.astype(BF16).astype(F32)
    xin = silu(taps(fields, small[3:7, :], slice(0, 256), 4))
    write = silu(taps(fields, small[7:11, 0:128], slice(256, 384), 4))
    seq_input[...] = xin
    seq_write[...] = write.astype(BF16)
    step = jnp.concatenate([by_position(dt_t, b * BLK) for b in range(NB)], axis=0)
    scaled = xin * per_head(step)
    weighted[...] = scaled.astype(BF16)
    state = jnp.zeros((128, 256), F32)
    before = jnp.zeros((1, 128), F32)
    for b in range(NB):
        rows = slice(b * BLK, (b + 1) * BLK)
        here = by_position(cum_t, b * BLK)
        end = here[BLK - 1 : BLK, :]
        local[b] = state.astype(BF16)
        to_end = per_head(jnp.exp(end - here))
        added = dot(write[rows].T.astype(BF16), (scaled[rows] * to_end).astype(BF16))
        state = state * per_head(jnp.exp(end - before)) + added
        before = end
    decay = per_head(jnp.exp(before))
    high = decay.astype(BF16).astype(F32)
    low = decay - high
    tail = jnp.where(
        lax.broadcasted_iota(jnp.int32, (8, 256), 0) < 4,
        jnp.broadcast_to(high, (8, 256)),
        jnp.broadcast_to(low, (8, 256)),
    ).astype(BF16)
    for j in range(8):
        pieces[j, 0:16, :] = state[16 * j : 16 * (j + 1)].astype(BF16)
        pieces[j, 16:24, :] = tail


def piece_of(ref, j):
    v = ref[j].astype(F32)
    return v[0:16], v[16:17] + v[20:21]


def plane_body(got, left, send):
    state = jnp.zeros((16, 256), F32)
    decay = jnp.ones((1, 256), F32)
    for j in range(8):
        s, d = piece_of(got, j)
        state = state * d + s
        decay = decay * d
    high = decay.astype(BF16).astype(F32)
    tail = jnp.where(
        lax.broadcasted_iota(jnp.int32, (8, 256), 0) < 4,
        jnp.broadcast_to(high, (8, 256)),
        jnp.broadcast_to(decay - high, (8, 256)),
    )
    second = lax.broadcasted_iota(jnp.int32, (8, 256), 0) == 1
    tail = jnp.where(second, jnp.broadcast_to(left[...], (8, 256)), tail)
    one = jnp.concatenate([state, tail], axis=0).astype(BF16)
    for k in range(16):
        send[k] = one


def enter_body(got, planes, out):
    z = lax.axis_index("z")
    state = jnp.zeros((16, 256), F32)
    lefts = []
    for k in range(16):
        lefts.append(planes[k].astype(F32)[17:18])
        s, d = piece_of(planes, k)
        state = jnp.where(k < z, state * d + s, state)
    left = jnp.concatenate(lefts, axis=0).astype(BF16)
    for j in range(8):
        out[j, 0:16, :] = state.astype(BF16)
        out[j, 16:32, :] = left
        s, d = piece_of(got, j)
        state = state * d + s


def rest_body(
    tok, halo, p0, p1, p2, p3, p4, p5, p6, p7, small,
    read_out, gate, mixer, wide,
    whole, more, laid, normed, fields, sem, sems, store_sem,
):
    parts = (p0, p1, p2, p3, p4, p5, p6, p7)
    fetch = fetches(tok, normed, sem)
    one = ring_copies(parts, FAR, whole, 0, 48, sems.at[0])
    two = ring_copies(parts, FAR, more, 48, 96, sems.at[1])
    three = ring_copies(parts, FAR, laid, 144, 64, sems.at[2])
    normed[0:HALO, :] = halo[...]
    lay_out(ring_pieces(parts, NEAR), ((whole, 0, 48), (more, 48, 96), (laid, 144, 64)))
    wait_for(fetch)
    wait_for(one)
    n = normed[...]

    def projected(ref, lo, count):
        return dot(n, blocks(ref, lo, count)).astype(BF16).astype(F32)

    fields[:, 0:128] = projected(whole, 0, 1)
    read_out[...] = silu(taps(fields, small[11:15, 0:128], slice(0, 128), 4)).astype(BF16)
    gate[...] = silu(projected(whole, 1, 2)[HALO:])
    wait_for(three)
    store = pltpu.make_async_copy(laid, wide, store_sem)
    store.start()
    wait_for(two)
    inner = projected(more, 2, 2)
    fields[...] = inner * projected(more, 4, 2)
    outer = projected(more, 0, 2)[HALO:]
    mixer[...] = (outer * taps(fields, small[0:3, :], slice(0, 256), 3)).astype(BF16)
    store.wait()


def within_body(
    read, far_weighted, far_input, far_write, far_local, cum_t, small, partly,
    weighted, seq_input, seq_write, local, sem,
):
    pairs = (
        (far_write, seq_write),
        (far_local, local),
        (far_weighted, weighted),
        (far_input, seq_input),
    )
    fetch = [
        pltpu.make_async_copy(far, here, sem.at[i]) for i, (far, here) in enumerate(pairs)
    ]
    for copy in fetch:
        copy.start()
    weight = per_head(small[16:17, 0:128])
    r = lax.broadcasted_iota(jnp.int32, (BLK, BLK), 0)
    s = lax.broadcasted_iota(jnp.int32, (BLK, BLK), 1)
    causal = r >= s
    low = s < 64
    before = jnp.zeros((1, 128), F32)
    wait_for(fetch)
    for b in range(NB):
        rows = slice(b * BLK, (b + 1) * BLK)
        rb = read[rows, :]
        scores = dot_nt(rb, seq_write[rows, :])
        here = by_position(cum_t, b * BLK)
        from_local = dot(rb, local[b]) * per_head(jnp.exp(here - before))
        before = here[BLK - 1 : BLK, :]
        halves = []
        for p in range(2):
            pair = weighted[rows, 128 * p : 128 * (p + 1)]
            two = []
            for h in (2 * p, 2 * p + 1):
                gap = here[:, h : h + 1] - cum_t[h : h + 1, rows]
                damped = scores * jnp.exp(jnp.where(causal, gap, -jnp.inf))
                two.append(dot(damped.astype(BF16), pair))
            halves.append(jnp.where(low, two[0], two[1]))
        within = jnp.concatenate(halves, axis=1)
        partly[rows, :] = within + from_local + weight * seq_input[rows, :]


def patch(wide, arriving):
    row = lax.broadcasted_iota(jnp.int32, (16, 128), 0)
    for j in range(8):
        lefts = arriving[j, 16:32, :].astype(F32)
        for z in range(16):
            tile = wide[z, j // 2, j % 2, 48:64, :].astype(F32)
            for i in range(2):
                v = lefts[z : z + 1, 128 * i : 128 * (i + 1)]
                tile = jnp.where(row == 14 + i, jnp.broadcast_to(v, (16, 128)), tile)
            wide[z, j // 2, j % 2, 48:64, :] = tile.astype(BF16)


def project_out(act, wide, out):
    a = act[...]
    for q in range(4):
        zs = slice(4 * q, 4 * (q + 1))
        w = [wide[zs, :, :, 16 * k : 16 * (k + 1), :].reshape(512, 128) for k in range(4)]
        w = jnp.concatenate(w, axis=1)
        out[:, 512 * q : 512 * (q + 1)] = dot_nt(a, w).astype(out.dtype)


def finish_rows(at, arriving, partly, read, gate, cum_t, mixer, small, act):
    rows = pl.ds(pl.multiple_of(at * 128, 128), 128)
    state = jnp.concatenate([arriving[j, 0:16, :] for j in range(8)], axis=0)
    part = cum_t[:, rows]
    here = jnp.concatenate([part, jnp.zeros((BLK - 8, BLK), F32)], axis=0).T
    head = partly[rows, :] + dot(read[rows, :], state) * per_head(jnp.exp(here))
    gated = head * gate[rows, :]
    square = gated * gated
    r = lax.broadcasted_iota(jnp.int32, (256, 256), 0) // 64
    s = lax.broadcasted_iota(jnp.int32, (256, 256), 1) // 64
    same = jnp.where(r == s, 1.0 / 64.0, 0.0).astype(BF16)
    high = square.astype(BF16)
    rest = (square - high.astype(F32)).astype(BF16)
    mean = dot(high, same) + dot(rest, same)
    act[:, 0:256] = mixer[rows, :]
    act[:, 256:512] = (gated * lax.rsqrt(mean + EPS) * small[15:16, :]).astype(BF16)


def tail_body(
    arriving, partly, read, gate, cum_t, mixer, small, stored, far, wide, act, sem
):
    fetch = pltpu.make_async_copy(stored, wide, sem)
    fetch.start()
    at = (lax.axis_index("tp") + 2) % 4
    finish_rows(at, arriving, partly, read, gate, cum_t, mixer, small, act)
    fetch.wait()
    patch(wide, arriving)
    project_out(act, wide, far)


def near_body(
    arriving, partly, read, gate, cum_t, mixer, small, wide, beside, near, mine, act
):
    y, c = lax.axis_index("tp"), lax.axis_index("c")
    for at, out in (((y + 3 + 2 * c) % 4, beside), ((y + 1 + 2 * c) % 4, near), (y, mine)):
        finish_rows(at, arriving, partly, read, gate, cum_t, mixer, small, act)
        project_out(act, wide, out)


def add_body(near, got, out):
    out[...] = (near[...].astype(F32) + got[...].astype(F32)).astype(BF16)


def sum_body(mine, a, b, out):
    v = mine[...].astype(F32) + a[...].astype(F32)
    out[...] = (v + b[...].astype(F32)).astype(BF16)


def exchanged(tiles, axis):
    return lax.all_to_all(tiles, axis, 0, 0, tiled=True)


def two_way(shard, axis, toward):
    steps = [(i, c, (i + (toward if c == 0 else -toward)) % 4) for i in range(4) for c in range(2)]
    if axis == "x":
        return lax.ppermute(shard, ("x", "c"), [(2 * i + c, 2 * j + c) for i, c, j in steps])
    return lax.ppermute(shard, ("c", "tp"), [(4 * c + i, 4 * c + j) for i, c, j in steps])


def swapped(shard):
    return lax.ppermute(shard, "c", [(0, 1), (1, 0)])


def per_device(
    tokens,
    input_norm_scale,
    outer_gate_weight,
    inner_gate_weight,
    value_weight_matrix,
    output_gate_weight,
    state_input_weight,
    write_key_weight,
    read_key_weight,
    step_size_weight,
    gated_conv_weight,
    input_conv_weight,
    write_conv_weight,
    read_conv_weight,
    step_size_bias,
    log_decay_rate,
    decay_spikes,
    direct_path_weight,
    head_norm_scale,
    conv_output_weight,
    state_output_weight,
):
    copied, own, left, small = call(
        prep_body,
        (
            shape((4, 128, 2048), BF16),
            shape((254, 128), BF16),
            shape((1, 256), F32),
            shape((24, 256), F32),
        ),
        (
            tokens,
            input_norm_scale.reshape(16, 128),
            state_input_weight,
            write_key_weight,
            read_key_weight,
            output_gate_weight,
            outer_gate_weight,
            inner_gate_weight,
            value_weight_matrix,
            conv_output_weight.T,
            state_output_weight.T,
            gated_conv_weight,
            input_conv_weight,
            write_conv_weight,
            read_conv_weight,
            head_norm_scale.reshape(2, 128),
            direct_path_weight[None],
            step_size_bias[None],
            log_decay_rate[None],
        ),
        mib=None,
    )
    tok = exchanged(copied, "tp")
    column = lax.all_gather(own, "z", axis=0, tiled=False)
    first, ring = call(
        cut_body,
        (main_memory((4, 16, 48, 128), BF16), main_memory((16, 208, 128), BF16)),
        (column,),
    )
    first = exchanged(first, "x")
    first_other = swapped(first)
    ring = [ring]
    ring.append(two_way(ring[0], "x", 1))
    ring.append(two_way(ring[0], "x", -1))
    ring.append(two_way(ring[1], "x", 1))
    ring += [swapped(part) for part in ring]
    dt_t, cum_t, edge = call(
        cum_body,
        (
            shape((8, ROWS), F32),
            shape((8, ROWS), F32),
            shape((HALO, 2048), BF16),
        ),
        (tok, step_size_weight.T, small, decay_spikes),
        scratch=(pltpu.VMEM((BLK, BLK), F32),),
    )
    halo = lax.ppermute(edge, SP, [(i, i + 1) for i in range(127)])
    weighted, seq_input, seq_write, local, pieces = call(
        first_body,
        (
            main_memory((ROWS, 256), BF16),
            main_memory((ROWS, 256), F32),
            main_memory((ROWS, 128), BF16),
            main_memory((NB, 128, 256), BF16),
            main_memory((8, 24, 256), BF16),
        ),
        (tok, halo, first, first_other, dt_t, cum_t, small),
        (
            pltpu.VMEM((16, 4, 2, 48, 128), BF16),
            pltpu.VMEM((HALO + ROWS, 2048), BF16),
            pltpu.VMEM((HALO + ROWS, 384), F32),
        ),
        mib=16,
    )
    got = exchanged(pieces, ("x", "c"))
    send = call(plane_body, shape((16, 24, 256), BF16), (got, left))
    planes = exchanged(send, "z")
    entering = call(enter_body, shape((8, 32, 256), BF16), (got, planes))
    arriving = exchanged(entering, ("x", "c"))

    read, gate, mixer, wide = call(
        rest_body,
        (
            on_chip((ROWS, 128), BF16),
            main_memory((ROWS, 256), F32),
            main_memory((ROWS, 256), BF16),
            main_memory((16, 4, 2, 64, 128), BF16),
        ),
        (tok, halo, *ring, small),
        scratch=(
            pltpu.VMEM((16, 4, 2, 48, 128), BF16),
            pltpu.VMEM((16, 4, 2, 96, 128), BF16),
            pltpu.VMEM((16, 4, 2, 64, 128), BF16),
            pltpu.VMEM((HALO + ROWS, 2048), BF16),
            pltpu.VMEM((HALO + ROWS, 256), F32),
            pltpu.SemaphoreType.DMA((4,)),
            pltpu.SemaphoreType.DMA((3, 8)),
            pltpu.SemaphoreType.DMA,
        ),
        mib=24,
        far_in=(0, *(2 + i for i in FAR)),
        far_out=(3,),
    )
    partly = call(
        within_body,
        shape((ROWS, 256), F32),
        (read, weighted, seq_input, seq_write, local, cum_t, small),
        scratch=(
            pltpu.VMEM((ROWS, 256), BF16),
            pltpu.VMEM((ROWS, 256), F32),
            pltpu.VMEM((ROWS, 128), BF16),
            pltpu.VMEM((NB, 128, 256), BF16),
            pltpu.SemaphoreType.DMA((4,)),
        ),
        far_in=(1, 2, 3, 4),
    )
    block_ = shape((128, 2048), BF16)
    rows_ = (arriving, partly, read, gate, cum_t, mixer, small)
    far, wide = call(
        tail_body,
        (block_, on_chip((16, 4, 2, 64, 128), BF16)),
        (*rows_, wide),
        scratch=(pltpu.VMEM((128, 512), BF16), pltpu.SemaphoreType.DMA),
        mib=16,
        far_in=(7,),
    )
    got_far = two_way(far, "tp", 1)
    beside, near, mine = call(
        near_body,
        (block_, block_, block_),
        (*rows_, wide),
        scratch=(pltpu.VMEM((128, 512), BF16),),
        mib=12,
    )
    got_beside = two_way(beside, "tp", -1)
    both = call(add_body, shape((128, 2048), BF16), (near, got_far))
    got_near = two_way(both, "tp", 1)
    return call(sum_body, shape((128, 2048), BF16), (mine, got_beside, got_near))


def solution(mesh):
    torus = Mesh(mesh.devices.reshape(16, 4, 2, mesh.shape["tp"]), SP_TP)
    rows = P(SP, "tp")
    cols = P("tp", SP)
    taps_ = P(None, "tp")
    heads = P("tp")
    return jax.shard_map(
        per_device,
        mesh=torus,
        in_specs=(
            P(SP_TP, None), P(), rows, rows, rows, rows, rows, rows, rows,
            taps_, taps_, taps_, taps_, taps_, heads, heads, cols, heads, heads, cols, cols,
        ),
        out_specs=P(SP_TP, None),
        check_vma=False,
    )
```
